32 devices in a mesh: sp: 8 (over z, x), tp: 4 (over y, core).
Axes of the slice: x: 2, y: 2, z: 4, core: 2. Of those that a mesh axis runs over, the one named last changes fastest.
Arguments:
- out_gate: bfloat16 [4096, 1536], P('sp', 'tp'), may hold values from -6 to 6
- in_gate: bfloat16 [4096, 1536], P('sp', 'tp'), may hold values from -6 to 6
- conv_values: bfloat16 [4096, 1536], P('sp', 'tp'), may hold values from -6 to 6
- conv_taps: float32 [3, 1536], P(None, 'tp'), may hold values from -3 to 3
- mix_gain: float32 [1536], replicated, may hold values from 0.1 to 1.9
- out_proj: bfloat16 [1536, 2048], replicated, may hold values from -0.15625 to 0.15625
- residual: bfloat16 [4096, 2048], P(('sp', 'tp')), may hold values from -6 to 6
- ffn_gain: float32 [2048], replicated, may hold values from 0.1 to 1.9
- routes: int32 [4096, 6], P(('sp', 'tp')), may hold values from 0 to 31, all different within a row; in each aligned block of 128 rows (0 to 127, 128 to 255, ...) at most 32 rows name the same one
- route_weights: float32 [4096, 6], P(('sp', 'tp')), may hold values from 0.05 to 1
- shared_gate: bfloat16 [2048, 512], replicated, may hold values from -0.125 to 0.125
- shared_up: bfloat16 [2048, 512], replicated, may hold values from -0.125 to 0.125
- shared_down: bfloat16 [512, 2048], replicated, may hold values from -0.25 to 0.25
- expert_gate: bfloat16 [32, 2048, 512], P(('sp', 'tp')), may hold values from -0.125 to 0.125
- expert_up: bfloat16 [32, 2048, 512], P(('sp', 'tp')), may hold values from -0.125 to 0.125
- expert_down: bfloat16 [32, 512, 2048], P(('sp', 'tp')), may hold values from -0.25 to 0.25
Outputs:
- layer_out: bfloat16 [4096, 2048], P(('sp', 'tp'))
The draws below stay inside these ranges and needn't reach their ends.
Inputs may be any that keep to these rules, and one draw needn't show every extreme that they name: `routes`: each row names 6 different experts. Within the rows of one device (aligned blocks of 128 rows) no expert is named more than 32 times, a bound that some block reaches.
All inputs are finite; a program needn't handle non-finite values.
Results may differ from the reference program's by a relative error of at most 0.0065.
Values may be sent and summed in bfloat16 or wider, within the bound.
A program may use at most 128 MiB of HBM per device.

```python
import math
import jax
import jax.numpy as jnp
import numpy as np
from jax import lax

D = 2048
DC = 1536
KERNEL = 3
FF_E = 512
FS = 512
TOP = 6
ROWS_DEV = 128
TOKENS = 4096
EXPERTS = 32
CAP = 32
N_SP = 8
N_TP = 4


def levels(key, shape, shards, smallest, largest):
    level = 1.0
    for axis_at, parts in shards:
        steps = jax.random.uniform(jax.random.fold_in(jax.random.fold_in(key, 6), axis_at), (parts,), jnp.float32, smallest / len(shards), largest / len(shards))
        level = level * jnp.repeat(jnp.exp(steps), shape[axis_at] // parts).reshape((-1,) + (1,) * (len(shape) - 1 - axis_at))
    return level


def deal_out(stream_key, own, number, rows, number_of, top, limit, slope):
    order = jax.random.permutation(stream_key, number_of)
    packed, common = portions_of(number_of, rows * top, limit, slope, True), portions_of(number_of, rows * top, limit, slope, False)
    places = jnp.arange(number_of)

    def named(sizes, offset_by):
        used = int((sizes > 0).sum())
        fixed = max(1, used // 4)
        passed = fixed + (places - fixed + offset_by * (used - fixed)) % max(1, number_of - fixed)
        return jnp.zeros((number_of,), jnp.int32).at[order[jnp.where(places < fixed, places, passed)]].set(jnp.asarray(sizes, jnp.int32))

    sizes = jnp.where(number % 4 == 0, named(packed, number // 4), named(common, number - number // 4 - 1))
    mixed = jax.random.permutation(jax.random.fold_in(own, 3), number_of)
    source_of, taker = mixed[0:number_of // 2 * 2:2], mixed[1:number_of // 2 * 2:2]
    margin = jnp.minimum(sizes[source_of] - 1, limit - sizes[taker]) // 2
    margin = jnp.where((source_of == order[0]) | (taker == order[0]) | (sizes[taker] == 0), 0, jnp.maximum(margin, 0))
    passed = jax.random.randint(jax.random.fold_in(own, 4), (number_of // 2,), 0, 1 << 20) % (margin + 1)
    sizes = sizes.at[source_of].add(-passed).at[taker].add(passed)
    labels = jnp.searchsorted(jnp.cumsum(sizes), jnp.arange(rows * top), side="right").astype(jnp.int32)
    listing = labels.reshape(top, rows).T
    listing = listing[jax.random.permutation(jax.random.fold_in(own, 1), rows)]
    offset_by = jax.random.randint(jax.random.fold_in(own, 2), (rows, 1), 0, top)
    return jnp.take_along_axis(listing, (jnp.arange(top)[None, :] + offset_by) % top, axis=1)


def portions_of(count, total, reach, slope, full):
    portions = [(1 << 20) // math.isqrt(rank ** slope) + 1 for rank in range(1, count + 1)]
    largest = reach if full else min(reach, max(-(-total // count), total * portions[0] // sum(portions)))
    least = 1 if total - largest >= count - 1 else 0
    given, surplus = [largest] + [least] * (count - 1), total - largest - least * (count - 1)
    while surplus > 0:
        movable = [i for i in range(1, count) if given[i] < largest] or [i for i in range(1, count) if given[i] < reach]
        whole, remaining = sum([portions[i] for i in movable]), surplus
        for i in movable:
            addition = min(reach - given[i], max(1, remaining * portions[i] // whole), surplus)
            given[i] = given[i] + addition
            surplus = surplus - addition
    return np.array(given)


def gaussian(own_key, shape, deviation, limit, split=(), kind=jnp.bfloat16):
    values = jax.random.normal(own_key, shape, jnp.float32) * deviation
    if len(split) > 0:
        values = levels(own_key, shape, split, -0.22, 0.18) * values
    return jnp.clip(values, min=-limit, max=limit).astype(kind)


def setup_inputs(seed: int = 0) -> dict:
    splits = jax.random.split(jax.random.key(seed), 17)
    out_gate = gaussian(splits[0], (TOKENS, DC), 1.0, 6.0, ((0, 8), (1, 4)))
    in_gate = gaussian(splits[1], (TOKENS, DC), 1.0, 6.0, ((0, 8), (1, 4)))
    conv_values = gaussian(splits[2], (TOKENS, DC), 1.0, 6.0, ((0, 8), (1, 4)))
    conv_taps = gaussian(splits[3], (KERNEL, DC), 0.6, 3.0, ((1, 4),), jnp.float32)
    mix_gain = jnp.clip(1.0 + 0.18 * jax.random.normal(splits[4], (DC,), jnp.float32), 0.1, 1.9)
    out_proj = gaussian(splits[5], (DC, D), DC ** -0.5, 0.15625)
    residual = gaussian(splits[6], (TOKENS, D), 1.0, 6.0, ((0, 32),))
    ffn_gain = jnp.clip(1.0 + 0.18 * jax.random.normal(splits[7], (D,), jnp.float32), 0.1, 1.9)
    routes_keys = jax.random.split(jax.random.fold_in(splits[8], 1), TOKENS // ROWS_DEV)
    routes_turns = jax.random.permutation(jax.random.fold_in(splits[8], 3), TOKENS // ROWS_DEV)
    routes = jax.vmap(lambda own, number: deal_out(jax.random.fold_in(splits[8], 2), own, number, ROWS_DEV, EXPERTS, TOP, CAP, 2))(routes_keys, routes_turns).reshape((TOKENS, TOP))
    route_weights = jnp.clip(jnp.exp(math.log(1.0) - 2.9957323 * jax.random.uniform(splits[9], (TOKENS, TOP), jnp.float32) ** levels(splits[9], (TOKENS, TOP), ((0, 32),), -0.2, 0.2)), 0.05, 1.0)
    shared_gate = gaussian(splits[10], (D, FS), D ** -0.5, 0.125)
    shared_up = gaussian(splits[11], (D, FS), D ** -0.5, 0.125)
    shared_down = gaussian(splits[12], (FS, D), FS ** -0.5, 0.25)
    expert_gate = gaussian(splits[13], (EXPERTS, D, FF_E), D ** -0.5, 0.125, ((0, 32),))
    expert_up = gaussian(splits[14], (EXPERTS, D, FF_E), D ** -0.5, 0.125, ((0, 32),))
    expert_down = gaussian(splits[15], (EXPERTS, FF_E, D), FF_E ** -0.5, 0.25, ((0, 32),))
    return dict(out_gate=out_gate, in_gate=in_gate, conv_values=conv_values, conv_taps=conv_taps, mix_gain=mix_gain, out_proj=out_proj, residual=residual, ffn_gain=ffn_gain, routes=routes, route_weights=route_weights, shared_gate=shared_gate, shared_up=shared_up, shared_down=shared_down, expert_gate=expert_gate, expert_up=expert_up, expert_down=expert_down)


def project_norm(conv_out, mix_gain, out_proj):
    values = conv_out.astype(jnp.float32)
    inverse = lax.rsqrt(lax.optimization_barrier(jnp.mean(values * values, axis=-1)) + 1e-06)
    scaled = (values * mix_gain).astype(jnp.bfloat16)
    return jnp.dot(scaled, out_proj, preferred_element_type=jnp.float32) * inverse[:, None]

def ffn_input(stream, ffn_gain):
    inverse = lax.rsqrt(lax.optimization_barrier(jnp.mean(stream * stream, axis=-1, keepdims=True)) + 1e-06)
    return (stream * inverse * ffn_gain).astype(jnp.bfloat16)

def swiglu_hidden(row_block, weight_gate, weight_up):
    gate_part = jnp.dot(row_block, weight_gate, preferred_element_type=jnp.float32)
    up_part = jnp.dot(row_block, weight_up, preferred_element_type=jnp.float32)
    return (jax.nn.silu(gate_part) * up_part).astype(jnp.bfloat16)

def reference(out_gate, in_gate, conv_values, conv_taps, mix_gain, out_proj, residual, ffn_gain, routes, route_weights, shared_gate, shared_up, shared_down, expert_gate, expert_up, expert_down):
    mixed_in = in_gate.astype(jnp.float32) * conv_values.astype(jnp.float32)
    taps_count = conv_taps.shape[0]
    length = mixed_in.shape[0]
    extended = jnp.concatenate([jnp.zeros((taps_count - 1, mixed_in.shape[1]), jnp.float32), mixed_in], axis=0)
    filtered = conv_taps[0] * extended[0:length]
    for offset in range(1, taps_count):
        filtered = filtered + conv_taps[offset] * extended[offset:offset + length]
    conv_out = (out_gate.astype(jnp.float32) * filtered).astype(jnp.bfloat16)
    stream = residual.astype(jnp.float32) + project_norm(conv_out, mix_gain, out_proj)
    normed = ffn_input(stream, ffn_gain)
    shared_result = jnp.dot(swiglu_hidden(normed, shared_gate, shared_up), shared_down, preferred_element_type=jnp.float32)
    top_count = routes.shape[1]
    token_count = routes.shape[0]
    model_width = normed.shape[1]
    flat_ids = routes.reshape(-1).astype(jnp.int32)
    gate_values = route_weights / lax.optimization_barrier(jnp.sum(route_weights, axis=1, keepdims=True)) * 2.5
    flat_gates = gate_values.reshape(-1)
    sort_order = jnp.argsort(flat_ids, stable=True).astype(jnp.int32)
    sorted_ids = flat_ids[sort_order]
    counts = jnp.bincount(flat_ids, length=EXPERTS).astype(jnp.int32)
    starts = (jnp.cumsum(counts) - counts).astype(jnp.int32)
    slot_rank = jnp.arange(flat_ids.shape[0], dtype=jnp.int32) - starts[sorted_ids]
    most_rows = N_SP * N_TP * CAP
    slot_index = (sorted_ids * most_rows + slot_rank).astype(jnp.int32)
    row_of = (sort_order // top_count).astype(jnp.int32)
    slot_rows = jnp.full((EXPERTS * most_rows,), token_count, jnp.int32).at[slot_index].set(row_of)
    slot_gates = jnp.zeros((EXPERTS * most_rows,), jnp.float32).at[slot_index].set(flat_gates[sort_order])
    padded = jnp.concatenate([normed, jnp.zeros((1, model_width), jnp.bfloat16)], axis=0)

    def add_expert(running, inputs):
        row_index, gate_slots, weight_gate, weight_up, weight_down = inputs
        picked = padded[row_index]
        hidden = swiglu_hidden(picked, weight_gate, weight_up)
        result = jnp.dot(hidden, weight_down, preferred_element_type=jnp.float32).astype(jnp.bfloat16)
        return (running.at[row_index].add(result.astype(jnp.float32) * gate_slots[:, None]), None)
    running = jnp.zeros((token_count + 1, model_width), jnp.float32)
    running, _ = lax.scan(add_expert, running, (slot_rows.reshape(EXPERTS, most_rows), slot_gates.reshape(EXPERTS, most_rows), expert_gate, expert_up, expert_down))
    routed = running[:token_count]
    return (stream + shared_result + routed).astype(jnp.bfloat16)
```

```python
import functools

import jax
import jax.numpy as jnp
from jax import lax
from jax.experimental import pallas as pl
from jax.experimental.pallas import tpu as pltpu
from jax.sharding import PartitionSpec as P

MESH = pl.DeviceIdType.MESH
META_ROWS = 16
HALO = 16


def ffn(x, gate, up, down):
    g = jnp.dot(x, gate[...], preferred_element_type=jnp.float32)
    u = jnp.dot(x, up[...], preferred_element_type=jnp.float32)
    h = (g / (1.0 + jnp.exp(-g)) * u).astype(jnp.bfloat16)
    return jnp.dot(h, down[...], preferred_element_type=jnp.float32)


def experts_kernel(
    n_sp, n_tp, lag, cap, top,
    og_hbm, ig_hbm, cv_hbm, taps, mix_gain, residual, ffn_gain, routes, route_weights,
    op_hbm, eg_hbm, eu_hbm, ed_hbm, sg_hbm, su_hbm, sd_hbm,
    out,
    og, ig, cv, conv_out, conv_in,
    gathered, metas, staged, arrived, results, returned,
    left_in, right_in, total,
    op, eg, eu, ed, sg, su, sd,
    w_sem, halo_send, halo_recv, conv_send, conv_recv,
    meta_send, meta_recv, ring_send, ring_recv,
    disp_send, disp_recv, ret_send, ret_recv, red_send, red_recv,
):
    sp = lax.axis_index("sp")
    tp = lax.axis_index("tp")
    half = n_sp // 2
    rows, width = total.shape
    length = og.shape[0]
    mid = rows // 2
    group = n_tp * cap
    wide = n_tp // 2
    batch = wide * cap
    depth = n_sp // wide
    x, z = lax.rem(sp, wide), lax.div(sp, wide)
    y, core = lax.div(tp, 2), lax.rem(tp, 2)

    def across(kind):
        return y + kind * (x - y)

    def along(kind):
        return x + kind * (y - x)

    def device_at(kind, ring_index, member_index):
        zz, aa = lax.div(ring_index, wide), lax.rem(ring_index, wide)
        bb, cc = lax.div(member_index, 2), lax.rem(member_index, 2)
        return zz * wide + aa + kind * (bb - aa), (bb + kind * (aa - bb)) * 2 + cc

    ring = z * wide + along(core)
    member = across(core) * 2 + core

    def place_of(index):
        a, zz = lax.rem(index, wide), lax.div(index, wide)
        return a * depth + zz + lax.rem(a, 2) * (depth - 1 - 2 * zz)

    def index_of(place):
        a, zz = lax.div(place, depth), lax.rem(place, depth)
        return (zz + lax.rem(a, 2) * (depth - 1 - 2 * zz)) * wide + a

    place = place_of(ring)

    def ahead(distance):
        return device_at(core, index_of(lax.rem(place + distance, n_sp)), member)

    right, left = ahead(1), ahead(n_sp - 1)

    barrier = pltpu.get_barrier_semaphore()

    def greet(device):
        pl.semaphore_signal(barrier, inc=1, device_id=device, device_id_type=MESH)

    for d in range(1, n_sp):
        greet(ahead(d))
    for j in range(1, n_tp):
        greet((sp, lax.rem(tp + j, n_tp)))
        greet(device_at(1, z * wide + y, lax.rem(x * 2 + core + j, n_tp)))
    greet((lax.rem(sp + 1, n_sp), tp))
    greet((lax.rem(sp + n_sp - 1, n_sp), tp))

    weights = [
        pltpu.make_async_copy(src, dst, w_sem.at[i])
        for i, (src, dst) in enumerate(
            ((ig_hbm, ig.at[pl.ds(HALO, length)]), (cv_hbm, cv.at[pl.ds(HALO, length)]),
             (og_hbm, og), (op_hbm, op), (sg_hbm, sg), (su_hbm, su), (sd_hbm, sd),
             (eg_hbm.at[0], eg), (eu_hbm.at[0], eu), (ed_hbm.at[0], ed))
        )
    ]
    for copy in weights[:4]:
        copy.start()

    def remote(src, dst, send, recv, device):
        return pltpu.make_async_remote_copy(
            src_ref=src, dst_ref=dst, send_sem=send, recv_sem=recv,
            device_id=device, device_id_type=MESH,
        )

    def meta_copy(d):
        return remote(metas.at[0], metas.at[d], meta_send.at[d], meta_recv.at[d], ahead(d))

    def part_of(h):
        return pl.ds(h * mid, mid)

    def ring_copy(s, way, h):
        dst = gathered.at[s + 1 if way == 0 else n_sp - s - 1, part_of(h)]
        src = gathered.at[s if way == 0 else lax.rem(n_sp - s, n_sp), part_of(h)]
        device = right if way == 0 else left
        return remote(src, dst, ring_send.at[way, s, h], ring_recv.at[way, s, h], device)

    def slots(index):
        return pl.ds(pl.multiple_of(index * cap, cap), cap)

    def disp_copy(p, j):
        to = lax.rem(member + j, n_tp)
        return remote(
            staged.at[p, slots(to)], arrived.at[core, slots(p * wide + across(core))],
            disp_send.at[p, j], disp_recv.at[core, p, across(core)], device_at(core, ring, to),
        )

    def is_own(kind, b):
        return jnp.logical_and(core == kind, across(kind) == b)

    def holder(kind, b):
        return device_at(kind, z * wide + along(kind), b * 2 + kind)

    def disp_arrival(kind, p, b):
        return remote(
            staged.at[p, slots(0)], arrived.at[kind, slots(p * wide + b)],
            disp_send.at[p, 0], disp_recv.at[kind, p, b], holder(kind, b),
        )

    def ret_copy(kind, p, b):
        me = across(kind) * 2 + core
        return remote(
            results.at[kind, slots(p * wide + b)], returned.at[p, slots(me)],
            ret_send.at[kind, p, b], ret_recv.at[p, me], holder(kind, b),
        )

    def ret_arrival(p, j):
        frm = lax.rem(member + j, n_tp)
        return remote(
            results.at[0, slots(0)], returned.at[p, slots(frm)],
            ret_send.at[0, p, 0], ret_recv.at[p, frm], device_at(core, ring, frm),
        )

    def red_copy(s, way, h):
        device = left if way == 0 else right
        src = gathered.at[s if way == 0 else n_sp - s, part_of(h)]
        dst = (left_in if way == 0 else right_in).at[s - 1, part_of(h)]
        return remote(src, dst, red_send.at[way, s, h], red_recv.at[way, s - 1, h], device)

    def halo_copy(i):
        buf = (ig, cv)[i]
        device = (lax.rem(sp + 1, n_sp), tp)
        return remote(
            buf.at[pl.ds(length, HALO)], buf.at[pl.ds(0, HALO)],
            halo_send.at[i], halo_recv.at[i], device,
        )

    def conv_copy(t):
        return remote(
            conv_out.at[t], conv_in.at[tp], conv_send.at[t], conv_recv.at[tp], (sp, t)
        )

    def conv_arrival(t):
        return remote(conv_out.at[t], conv_in.at[t], conv_send.at[t], conv_recv.at[t], (sp, t))

    experts_total = n_sp * n_tp
    expert = lax.broadcasted_iota(jnp.int32, (experts_total, rows), 0)
    named = [routes[k : k + 1, :] == expert for k in range(top)]
    onehot = jnp.zeros((experts_total, rows), jnp.float32)
    for hit in named:
        onehot = jnp.where(hit, 1.0, onehot)
    earlier = lax.broadcasted_iota(jnp.int32, (rows, rows), 0) < lax.broadcasted_iota(
        jnp.int32, (rows, rows), 1
    )
    before = jnp.dot(
        onehot.astype(jnp.bfloat16),
        jnp.where(earlier, 1.0, 0.0).astype(jnp.bfloat16),
        preferred_element_type=jnp.float32,
    )

    def split(value, by):
        high = jnp.floor((value + 0.5) / by)
        return high, value - high * by

    rest, ec = split(expert.astype(jnp.float32), 2)
    rest, ey = split(rest, wide)
    ez, ex = split(rest, wide)
    turn = core.astype(jnp.float32)
    ea, eb = ex + turn * (ey - ex), ey + turn * (ex - ey)
    slot = before + ((ez * wide + ea) * n_tp + eb * 2 + ec) * cap
    metas[0] = jnp.zeros(metas.shape[1:], jnp.float32)
    for k in range(top):
        metas[0, k : k + 1, :] = jnp.sum(jnp.where(named[k], slot, 0.0), axis=0, keepdims=True)
    weight = route_weights[...]
    metas[0, top : 2 * top, :] = weight / jnp.sum(weight, axis=0, keepdims=True) * 2.5

    for copy in weights[:3]:
        copy.wait()
    with jax.named_scope("barrier"):
        pl.semaphore_wait(barrier, n_sp - 1 + 2 * (n_tp - 1) + 2)
    halo_copy(0).start()
    halo_copy(1).start()
    for copy in weights[4:7]:
        copy.start()

    taps_count = taps.shape[0]
    owners = [t for t in range(2, n_tp, 2)] + [t for t in range(1, n_tp, 2)] + [0]
    for t in owners:
        if t == 0:
            with jax.named_scope("halo_wait"):
                halo_copy(0).wait_recv()
                halo_copy(1).wait_recv()
        span = pl.ds(t * rows, rows + HALO)
        mixed = ig[span].astype(jnp.float32) * cv[span].astype(jnp.float32)
        if t == 0:
            blank = jnp.where(sp == 0, HALO, 0)
            at = lax.broadcasted_iota(jnp.int32, mixed.shape, 0)
            mixed = jnp.where(at >= blank, mixed, 0.0)
        base = HALO - (taps_count - 1)
        filtered = taps[0:1, :] * mixed[base : base + rows]
        for o in range(1, taps_count):
            filtered = filtered + taps[o : o + 1, :] * mixed[base + o : base + o + rows]
        value = (og[pl.ds(t * rows, rows)].astype(jnp.float32) * filtered).astype(jnp.bfloat16)
        conv_out[t] = value

        @pl.when(tp != t)
        def _():
            conv_copy(t).start()

    for d in range(1, n_sp):
        meta_copy(d).start()
    weights[3].wait()
    for copy in weights[7:]:
        copy.start()

    squares = jnp.zeros((rows, 1), jnp.float32)
    product = jnp.zeros((rows, width), jnp.float32)
    part_width = conv_in.shape[2]
    sources = [tp, tp + 1 - 2 * core]
    for i in range(1, wide):
        other = lax.rem(y + i, wide) * 2
        sources += [other, other + 1]
    for i, t in enumerate(sources):
        if i == 0:
            value = conv_out[t].astype(jnp.float32)
        else:
            with jax.named_scope("conv_wait"):
                conv_arrival(t).wait_recv()
            value = conv_in[t].astype(jnp.float32)
        gain = mix_gain[:, :part_width]
        for k in range(1, n_tp):
            gain = jnp.where(t == k, mix_gain[:, k * part_width : (k + 1) * part_width], gain)
        squares = squares + jnp.sum(value * value, axis=1, keepdims=True)
        product = product + jnp.dot(
            (value * gain).astype(jnp.bfloat16),
            op[pl.ds(pl.multiple_of(t * part_width, part_width), part_width), :],
            preferred_element_type=jnp.float32,
        )
    inverse = lax.rsqrt(squares / (n_tp * part_width) + 1e-06)
    stream = residual[...].astype(jnp.float32) + product * inverse
    power = jnp.mean(stream * stream, axis=1, keepdims=True)
    gathered[0] = (stream * lax.rsqrt(power + 1e-06) * ffn_gain[...]).astype(jnp.bfloat16)
    total[...] = stream

    first_slot = (ring * group).astype(jnp.float32)

    def matches(meta, k):
        at = lax.broadcasted_iota(jnp.int32, (group, rows), 0).astype(jnp.float32) + first_slot
        return at == meta[k : k + 1, :]

    def dispatch(d, p):
        meta = metas[d]
        pick = jnp.zeros((group, rows), jnp.float32)
        for k in range(top):
            pick = jnp.where(matches(meta, k), 1.0, pick)
        staged[p] = jnp.dot(
            pick.astype(jnp.bfloat16), gathered[d], preferred_element_type=jnp.float32
        ).astype(jnp.bfloat16)
        for j in range(1, n_tp):
            disp_copy(p, j).start()
        arrived[core, slots(p * wide + across(core))] = staged[p, slots(member)]

    def gather_action(a):
        @pl.when(a == 0)
        def _():
            for h in range(2):
                for way in range(2):
                    ring_copy(0, way, way if h == 0 else 1 - way).start()

        @pl.when(a > 0)
        def _():
            for way in range(2):
                with jax.named_scope("ring_wait"):
                    ring_copy(a - 1, way, way).wait_recv()

                @pl.when(a < half)
                def _():
                    ring_copy(a, way, way).start()

            @pl.when(a < half)
            def _():
                for way in range(2):
                    with jax.named_scope("ring_wait"):
                        ring_copy(a - 1, way, 1 - way).wait_recv()

                    @pl.when(a < half - 1)
                    def _():
                        ring_copy(a, way, 1 - way).start()

        def one(i, c):
            d = a + i * (n_sp - 2 * a)

            @pl.when(d > 0)
            def _():
                meta_copy(d).wait_recv()

            with jax.named_scope("dispatch"):
                dispatch(d, jnp.maximum(2 * a - 1, 0) + i)
            return c

        count = jnp.where(jnp.logical_or(a == 0, a == half), 1, 2)
        lax.fori_loop(0, count, one, 0)

    def run_expert(kind, p, count):
        with jax.named_scope("disp_wait"):
            for i in range(count):
                for b in range(wide):
                    @pl.when(jnp.logical_not(is_own(kind, b)))
                    def _():
                        disp_arrival(kind, p + i, b).wait_recv()

        span = pl.ds(pl.multiple_of(p * batch, batch), count * batch)
        with jax.named_scope("ffn"):
            results[kind, span] = ffn(arrived[kind, span], eg, eu, ed).astype(jnp.bfloat16)

    def give_back(kind, p):
        for b in range(wide):
            own = is_own(kind, b)

            @pl.when(jnp.logical_not(own))
            def _():
                ret_copy(kind, p, b).start()

            @pl.when(own)
            def _():
                returned[p, slots(member)] = results[kind, slots(p * wide + b)]

    def expert_action(kind, u):
        @pl.when(jnp.logical_and(u > 1, u <= half))
        def _():
            run_expert(kind, 2 * u - 3, 2)

        @pl.when(jnp.logical_or(u == 1, u == half))
        def _():
            run_expert(kind, jnp.where(u == 1, 0, n_sp - 1), 1)

        @pl.when(u == half)
        def _():
            give_back(kind, n_sp - 1)

        @pl.when(jnp.logical_and(u >= half, u <= 2 * half - 2))
        def _():
            give_back(kind, 4 * half - 3 - 2 * u)
            give_back(kind, 4 * half - 2 - 2 * u)

        @pl.when(u == 2 * half - 2)
        def _():
            give_back(kind, 0)

    def combine(d, p):
        with jax.named_scope("ret_wait"):
            for j in range(1, n_tp):
                ret_arrival(p, j).wait_recv()
        meta = metas[d]
        mix = jnp.zeros((group, rows), jnp.float32)
        for k in range(top):
            mix = jnp.where(matches(meta, k), meta[top + k : top + k + 1, :], mix)
        return lax.dot_general(
            mix.astype(jnp.bfloat16), returned[p], (((0,), (0,)), ((), ())),
            preferred_element_type=jnp.float32,
        )

    def reduce_start():
        for way in range(2):
            for h in range(2):
                for s in range(half - 1 if h != way else half):
                    ring_copy(s, way, h).wait_send()
        gathered[half] = combine(half, n_sp - 1).astype(jnp.bfloat16)
        red_copy(half, 0, 0).start()
        red_copy(half, 1, 1).start()

    def reduce_step(s):
        for way, buf_in in enumerate((left_in, right_in)):
            d, p = (s, 2 * s - 1) if way == 0 else (n_sp - s, 2 * s)
            part = combine(d, p)
            for order in range(2):
                h = way if order == 0 else 1 - way
                if order == 0:
                    with jax.named_scope("red_wait"):
                        red_copy(s + 1, way, h).wait_recv()
                else:

                    @pl.when(s < half - 1)
                    def _():
                        with jax.named_scope("red_wait2"):
                            red_copy(s + 1, way, h).wait_recv()

                at = slice(h * mid, (h + 1) * mid)
                gathered[d, at] = (part[at] + buf_in[s, at].astype(jnp.float32)).astype(
                    jnp.bfloat16
                )
                red_copy(s, way, h).start()

    def finish():
        part = combine(0, 0) + total[...]
        for way, buf_in in enumerate((left_in, right_in)):
            with jax.named_scope("red_wait_last"):
                for h in range(2):
                    red_copy(1, way, h).wait_recv()
            part = part + buf_in[0].astype(jnp.float32)
        out[...] = part.astype(out.dtype)

    left_in[half - 1, mid:] = jnp.zeros((rows - mid, width), jnp.bfloat16)
    right_in[half - 1, :mid] = jnp.zeros((mid, width), jnp.bfloat16)

    def step(k, carry):
        a = k - lag * core

        @pl.when(jnp.logical_and(a >= 0, a <= half))
        def _():
            gather_action(a)

        @pl.when(k == 0)
        def _():
            for copy in weights[4:7]:
                copy.wait()
            with jax.named_scope("shared"):
                total[...] += ffn(gathered[0], sg, su, sd)
            for copy in weights[7:]:
                copy.wait()

        def kinds(kind, c):
            expert_action(kind, k - lag * kind)
            return c

        lax.fori_loop(0, 2, kinds, 0)

        @pl.when(a == half + 1)
        def _():
            reduce_start()

        @pl.when(jnp.logical_and(a > half + 1, a <= 2 * half))
        def _():
            reduce_step(2 * half + 1 - a)

        @pl.when(a == 2 * half + 1)
        def _():
            finish()

        return carry

    lax.fori_loop(0, lag + 2 * half + 2, step, 0)

    for d in range(1, n_sp):
        meta_copy(d).wait_send()
    for t in range(n_tp):

        @pl.when(tp != t)
        def _():
            conv_copy(t).wait_send()

    for way in range(2):
        halo_copy(way).wait_send()
        red_copy(half, way, way).wait_send()
        for s in range(1, half):
            for h in range(2):
                red_copy(s, way, h).wait_send()

    def drain(p, c):
        for j in range(1, n_tp):
            disp_copy(p, j).wait_send()
        for kind in range(2):
            for b in range(wide):

                @pl.when(jnp.logical_not(is_own(kind, b)))
                def _():
                    ret_copy(kind, p, b).wait_send()

        return c

    lax.fori_loop(0, n_sp, drain, 0)


def body(
    out_gate,
    in_gate,
    conv_values,
    conv_taps,
    mix_gain,
    out_proj,
    residual,
    ffn_gain,
    routes,
    route_weights,
    shared_gate,
    shared_up,
    shared_down,
    expert_gate,
    expert_up,
    expert_down,
):
    n_sp, n_tp = lax.axis_size("sp"), lax.axis_size("tp")
    length, channels = in_gate.shape
    rows, width = residual.shape
    top = routes.shape[1]
    cap = max(2, 4 * rows * top // (3 * n_sp * n_tp))
    hidden, shared_hidden = expert_gate.shape[-1], shared_gate.shape[-1]
    half = n_sp // 2
    group = n_tp * cap
    wide = n_tp // 2
    lag = 0
    bf, f32 = jnp.bfloat16, jnp.float32
    vmem = pl.BlockSpec(memory_space=pltpu.VMEM)
    anywhere = pl.BlockSpec(memory_space=pl.ANY)
    dma = pltpu.SemaphoreType.DMA
    return pl.pallas_call(
        functools.partial(experts_kernel, n_sp, n_tp, lag, cap, top),
        out_shape=jax.ShapeDtypeStruct((rows, width), bf),
        in_specs=[anywhere] * 3 + [vmem] * 6 + [anywhere] * 7,
        out_specs=vmem,
        scratch_shapes=[
            pltpu.VMEM((length, channels), bf),
            pltpu.VMEM((length + HALO, channels), bf),
            pltpu.VMEM((length + HALO, channels), bf),
            pltpu.VMEM((n_tp, rows, channels), bf),
            pltpu.VMEM((n_tp, rows, channels), bf),
            pltpu.VMEM((n_sp, rows, width), bf),
            pltpu.VMEM((n_sp, META_ROWS, rows), f32),
            pltpu.VMEM((n_sp, group, width), bf),
            pltpu.VMEM((2, n_sp * wide * cap, width), bf),
            pltpu.VMEM((2, n_sp * wide * cap, width), bf),
            pltpu.VMEM((n_sp, group, width), bf),
            pltpu.VMEM((half, rows, width), bf),
            pltpu.VMEM((half, rows, width), bf),
            pltpu.VMEM((rows, width), f32),
            pltpu.VMEM((n_tp * channels, width), bf),
            pltpu.VMEM((width, hidden), bf),
            pltpu.VMEM((width, hidden), bf),
            pltpu.VMEM((hidden, width), bf),
            pltpu.VMEM((width, shared_hidden), bf),
            pltpu.VMEM((width, shared_hidden), bf),
            pltpu.VMEM((shared_hidden, width), bf),
            dma((10,)),
            dma((2,)),
            dma((2,)),
            dma((n_tp,)),
            dma((n_tp,)),
            dma((n_sp,)),
            dma((n_sp,)),
            dma((2, half, 2)),
            dma((2, half, 2)),
            dma((n_sp, n_tp)),
            dma((2, n_sp, wide)),
            dma((2, n_sp, wide)),
            dma((n_sp, n_tp)),
            dma((2, half + 1, 2)),
            dma((2, half + 1, 2)),
        ],
        compiler_params=pltpu.CompilerParams(
            collective_id=0, has_side_effects=True, vmem_limit_bytes=63 * 1024 * 1024
        ),
    )(
        out_gate, in_gate, conv_values, conv_taps, mix_gain.reshape(1, n_tp * channels),
        residual, ffn_gain.reshape(1, width), routes.T, route_weights.T,
        out_proj, expert_gate, expert_up, expert_down, shared_gate, shared_up, shared_down,
    )


def solution(mesh):
    in_specs = (
        P("sp", "tp"),
        P("sp", "tp"),
        P("sp", "tp"),
        P(None, "tp"),
        P(),
        P(),
        P(("sp", "tp"), None),
        P(),
        P(("sp", "tp"), None),
        P(("sp", "tp"), None),
        P(),
        P(),
        P(),
        P(("sp", "tp"), None, None),
        P(("sp", "tp"), None, None),
        P(("sp", "tp"), None, None),
    )
    out_specs = P(("sp", "tp"), None)
    return jax.shard_map(body, mesh=mesh, in_specs=in_specs, out_specs=out_specs, check_vma=False)
```

```python
import functools

import jax
import jax.numpy as jnp
from jax import lax
from jax.experimental import pallas as pl
from jax.experimental.pallas import tpu as pltpu
from jax.sharding import PartitionSpec as P

MESH = pl.DeviceIdType.MESH
META_ROWS = 16
HALO = 16


def ffn(x, gate, up, down):
    g = jnp.dot(x, gate[...], preferred_element_type=jnp.float32)
    u = jnp.dot(x, up[...], preferred_element_type=jnp.float32)
    h = (g / (1.0 + jnp.exp(-g)) * u).astype(jnp.bfloat16)
    return jnp.dot(h, down[...], preferred_element_type=jnp.float32)


def experts_kernel(
    n_sp, n_tp, cap, top,
    og_hbm, ig_hbm, cv_hbm, taps_hbm, mix_gain_hbm, residual_hbm, ffn_gain_hbm,
    routes_hbm, route_weights_hbm, op_hbm, eg_hbm, eu_hbm, ed_hbm, sg_hbm, su_hbm, sd_hbm,
    out,
    taps, mix_gain, residual, ffn_gain, routes, route_weights, result,
    og, ig, cv, conv_out, conv_in,
    gathered, metas, staged, arrived, results, returned,
    left_in, right_in, total, parts,
    op, eg, eu, ed, sg, su, sd,
    w_sem, small_sem, out_sem, halo_send, halo_recv, conv_send, conv_recv,
    meta_send, meta_recv, ring_send, ring_recv,
    disp_send, disp_recv, ret_send, ret_recv, red_send, red_recv,
):
    sp = lax.axis_index("sp")
    tp = lax.axis_index("tp")
    half = n_sp // 2
    rows, width = total.shape
    length = og.shape[0]
    mid = rows // 2
    group = n_tp * cap
    wide = n_tp // 2
    batch = wide * cap
    depth = n_sp // wide
    x, z = lax.rem(sp, wide), lax.div(sp, wide)
    y, core = lax.div(tp, 2), lax.rem(tp, 2)

    def across(kind):
        return y + kind * (x - y)

    def along(kind):
        return x + kind * (y - x)

    def device_at(kind, ring_index, member_index):
        zz, aa = lax.div(ring_index, wide), lax.rem(ring_index, wide)
        bb, cc = lax.div(member_index, 2), lax.rem(member_index, 2)
        return zz * wide + aa + kind * (bb - aa), (bb + kind * (aa - bb)) * 2 + cc

    ring = z * wide + along(core)
    member = across(core) * 2 + core

    def place_of(index):
        a, zz = lax.rem(index, wide), lax.div(index, wide)
        return a * depth + zz + lax.rem(a, 2) * (depth - 1 - 2 * zz)

    def index_of(place):
        a, zz = lax.div(place, depth), lax.rem(place, depth)
        return (zz + lax.rem(a, 2) * (depth - 1 - 2 * zz)) * wide + a

    place = place_of(ring)

    def ahead(distance):
        return device_at(core, index_of(lax.rem(place + distance, n_sp)), member)

    right, left = ahead(1), ahead(n_sp - 1)

    barrier = pltpu.get_barrier_semaphore()

    def greet(device):
        pl.semaphore_signal(barrier, inc=1, device_id=device, device_id_type=MESH)

    greet(right)
    greet(left)
    for j in range(1, n_tp):
        greet((sp, lax.rem(tp + j, n_tp)))
        greet(device_at(1, z * wide + y, lax.rem(x * 2 + core + j, n_tp)))
    greet((lax.rem(sp + 1, n_sp), tp))
    greet((lax.rem(sp + n_sp - 1, n_sp), tp))

    weights = [
        pltpu.make_async_copy(src, dst, w_sem.at[i])
        for i, (src, dst) in enumerate(
            ((ig_hbm, ig.at[pl.ds(HALO, length)]), (cv_hbm, cv.at[pl.ds(HALO, length)]),
             (og_hbm, og), (op_hbm, op), (sg_hbm, sg), (su_hbm, su), (sd_hbm, sd),
             (eg_hbm.at[0], eg), (eu_hbm.at[0], eu), (ed_hbm.at[0], ed))
        )
    ]
    smalls = [
        pltpu.make_async_copy(src, dst, small_sem.at[i])
        for i, (src, dst) in enumerate(
            ((taps_hbm, taps), (routes_hbm, routes), (route_weights_hbm, route_weights),
             (mix_gain_hbm, mix_gain), (ffn_gain_hbm, ffn_gain), (residual_hbm, residual))
        )
    ]
    for copy in weights[:2] + smalls[:1] + weights[2:3] + smalls[1:] + weights[3:4]:
        copy.start()

    def remote(src, dst, send, recv, device):
        return pltpu.make_async_remote_copy(
            src_ref=src, dst_ref=dst, send_sem=send, recv_sem=recv,
            device_id=device, device_id_type=MESH,
        )

    def meta_copy(s, way):
        dst = metas.at[s + 1 if way == 0 else n_sp - s - 1]
        src = metas.at[s if way == 0 else lax.rem(n_sp - s, n_sp)]
        device = right if way == 0 else left
        return remote(src, dst, meta_send.at[way, s], meta_recv.at[way, s], device)

    def part_of(h):
        return pl.ds(h * mid, mid)

    def ring_copy(s, way, h):
        dst = gathered.at[s + 1 if way == 0 else n_sp - s - 1, part_of(h)]
        src = gathered.at[s if way == 0 else lax.rem(n_sp - s, n_sp), part_of(h)]
        device = right if way == 0 else left
        return remote(src, dst, ring_send.at[way, s, h], ring_recv.at[way, s, h], device)

    def slots(index):
        return pl.ds(pl.multiple_of(index * cap, cap), cap)

    def row_of(kind, p, b):
        return slots((p * 2 + kind) * wide + b)

    def disp_copy(p, j):
        to = lax.rem(member + j, n_tp)
        return remote(
            staged.at[p, slots(to)], arrived.at[row_of(core, p, across(core))],
            disp_send.at[p, j], disp_recv.at[core, p, across(core)], device_at(core, ring, to),
        )

    def is_own(kind, b):
        return jnp.logical_and(core == kind, across(kind) == b)

    def holder(kind, b):
        return device_at(kind, z * wide + along(kind), b * 2 + kind)

    def disp_arrival(kind, p, b):
        return remote(
            staged.at[p, slots(0)], arrived.at[row_of(kind, p, b)],
            disp_send.at[p, 0], disp_recv.at[kind, p, b], holder(kind, b),
        )

    def ret_copy(kind, p, b):
        me = across(kind) * 2 + core
        return remote(
            results.at[row_of(kind, p, b)], returned.at[p, slots(me)],
            ret_send.at[kind, p, b], ret_recv.at[p, me], holder(kind, b),
        )

    def ret_arrival(p, j):
        frm = lax.rem(member + j, n_tp)
        return remote(
            results.at[slots(0)], returned.at[p, slots(frm)],
            ret_send.at[0, p, 0], ret_recv.at[p, frm], device_at(core, ring, frm),
        )

    def red_copy(s, way, h):
        device = left if way == 0 else right
        src = gathered.at[s if way == 0 else n_sp - s, part_of(h)]
        dst = (left_in if way == 0 else right_in).at[s - 1, part_of(h)]
        return remote(src, dst, red_send.at[way, s, h], red_recv.at[way, s - 1, h], device)

    def halo_copy(i):
        buf = (ig, cv)[i]
        device = (lax.rem(sp + 1, n_sp), tp)
        return remote(
            buf.at[pl.ds(length, HALO)], buf.at[pl.ds(0, HALO)],
            halo_send.at[i], halo_recv.at[i], device,
        )

    pieces = (pl.ds(0, HALO), pl.ds(HALO, rows - HALO))

    def conv_copy(t, i):
        return remote(
            conv_out.at[t, pieces[i]], conv_in.at[tp, pieces[i]],
            conv_send.at[t, i], conv_recv.at[tp, i], (sp, t),
        )

    def conv_arrival(t, i):
        return remote(
            conv_out.at[t, pieces[i]], conv_in.at[t, pieces[i]],
            conv_send.at[t, i], conv_recv.at[t, i], (sp, t),
        )

    taps_count = taps.shape[0]

    def convolve(t, first, count):
        span = pl.ds(t * rows + first, count + HALO)
        mixed = ig[span].astype(jnp.float32) * cv[span].astype(jnp.float32)
        if t == 0 and first == 0:
            blank = jnp.where(sp == 0, HALO, 0)
            at = lax.broadcasted_iota(jnp.int32, mixed.shape, 0)
            mixed = jnp.where(at >= blank, mixed, 0.0)
        base = HALO - (taps_count - 1)
        filtered = taps[0:1, :] * mixed[base : base + count]
        for o in range(1, taps_count):
            filtered = filtered + taps[o : o + 1, :] * mixed[base + o : base + o + count]
        gate = og[pl.ds(t * rows + first, count)].astype(jnp.float32)
        conv_out[t, pl.ds(first, count)] = (gate * filtered).astype(jnp.bfloat16)

    def send_conv(t, some):
        @pl.when(tp != t)
        def _():
            for i in some:
                conv_copy(t, i).start()

    owners = [t for t in range(2, n_tp, 2)] + [t for t in range(1, n_tp, 2)]
    for copy in weights[:3] + smalls[:1]:
        copy.wait()
    for t in owners:
        convolve(t, 0, rows)
    convolve(0, HALO, rows - HALO)
    with jax.named_scope("barrier"):
        pl.semaphore_wait(barrier, 2 + 2 * (n_tp - 1) + 2)
    halo_copy(0).start()
    halo_copy(1).start()
    for t in owners:
        send_conv(t, (1, 0))
    send_conv(0, (1,))
    for copy in weights[4:7]:
        copy.start()
    for copy in smalls[1:]:
        copy.wait()

    experts_total = n_sp * n_tp
    expert = lax.broadcasted_iota(jnp.int32, (experts_total, rows), 0)
    named = [routes[k : k + 1, :] == expert for k in range(top)]
    onehot = jnp.zeros((experts_total, rows), jnp.float32)
    for hit in named:
        onehot = jnp.where(hit, 1.0, onehot)
    earlier = lax.broadcasted_iota(jnp.int32, (rows, rows), 0) < lax.broadcasted_iota(
        jnp.int32, (rows, rows), 1
    )
    before = jnp.dot(
        onehot.astype(jnp.bfloat16),
        jnp.where(earlier, 1.0, 0.0).astype(jnp.bfloat16),
        preferred_element_type=jnp.float32,
    )

    def split(value, by):
        high = jnp.floor((value + 0.5) / by)
        return high, value - high * by

    rest, ec = split(expert.astype(jnp.float32), 2)
    rest, ey = split(rest, wide)
    ez, ex = split(rest, wide)
    turn = core.astype(jnp.float32)
    ea, eb = ex + turn * (ey - ex), ey + turn * (ex - ey)
    slot = before + ((ez * wide + ea) * n_tp + eb * 2 + ec) * cap
    metas[0] = jnp.zeros(metas.shape[1:], jnp.float32)
    for k in range(top):
        metas[0, k : k + 1, :] = jnp.sum(jnp.where(named[k], slot, 0.0), axis=0, keepdims=True)
    weight = route_weights[...]
    metas[0, top : 2 * top, :] = weight / jnp.sum(weight, axis=0, keepdims=True) * 2.5

    with jax.named_scope("halo_wait"):
        halo_copy(0).wait_recv()
        halo_copy(1).wait_recv()
    convolve(0, 0, HALO)
    send_conv(0, (0,))
    weights[3].wait()
    for copy in weights[7:]:
        copy.start()

    squares = jnp.zeros((rows, 1), jnp.float32)
    product = jnp.zeros((rows, width), jnp.float32)
    part_width = conv_in.shape[2]
    gains = mix_gain[...].reshape(1, n_tp * part_width)
    sources = [tp, tp + 1 - 2 * core]
    for i in range(1, wide):
        other = lax.rem(y + i, wide) * 2
        sources += [other, other + 1]
    for i, t in enumerate(sources):
        if i == 0:
            value = conv_out[t].astype(jnp.float32)
        else:
            with jax.named_scope("conv_wait"):
                for i in range(2):
                    conv_arrival(t, i).wait_recv()
            value = conv_in[t].astype(jnp.float32)
        gain = gains[:, :part_width]
        for k in range(1, n_tp):
            gain = jnp.where(t == k, gains[:, k * part_width : (k + 1) * part_width], gain)
        squares = squares + jnp.sum(value * value, axis=1, keepdims=True)
        product = product + jnp.dot(
            (value * gain).astype(jnp.bfloat16),
            op[pl.ds(pl.multiple_of(t * part_width, part_width), part_width), :],
            preferred_element_type=jnp.float32,
        )
    inverse = lax.rsqrt(squares / (n_tp * part_width) + 1e-06)
    stream = residual[...].astype(jnp.float32) + product * inverse
    power = jnp.mean(stream * stream, axis=1, keepdims=True)
    gathered[0] = (stream * lax.rsqrt(power + 1e-06) * ffn_gain[...]).astype(jnp.bfloat16)
    total[...] = stream

    first_slot = (ring * group).astype(jnp.float32)

    def matches(meta, k):
        at = lax.broadcasted_iota(jnp.int32, (group, rows), 0).astype(jnp.float32) + first_slot
        return at == meta[k : k + 1, :]

    def dispatch(d, p):
        meta = metas[d]
        pick = jnp.zeros((group, rows), jnp.float32)
        for k in range(top):
            pick = jnp.where(matches(meta, k), 1.0, pick)
        staged[p] = jnp.dot(
            pick.astype(jnp.bfloat16), gathered[d], preferred_element_type=jnp.float32
        ).astype(jnp.bfloat16)
        for j in range(1, n_tp):
            disp_copy(p, j).start()
        arrived[row_of(core, p, across(core))] = staged[p, slots(member)]

    def gather_action(a):
        @pl.when(a == 0)
        def _():
            for h in range(2):
                for way in range(2):
                    if h == 0:
                        meta_copy(0, way).start()
                    ring_copy(0, way, way if h == 0 else 1 - way).start()

        @pl.when(a > 0)
        def _():
            meta_copy(a - 1, 0).wait_recv()

            @pl.when(a < half)
            def _():
                meta_copy(a, 0).start()
                meta_copy(a - 1, 1).wait_recv()

            @pl.when(a < half - 1)
            def _():
                meta_copy(a, 1).start()

            for way in range(2):
                with jax.named_scope("ring_wait"):
                    ring_copy(a - 1, way, way).wait_recv()

                @pl.when(a < half)
                def _():
                    ring_copy(a, way, way).start()

            @pl.when(a < half)
            def _():
                for way in range(2):
                    with jax.named_scope("ring_wait"):
                        ring_copy(a - 1, way, 1 - way).wait_recv()

                    @pl.when(a < half - 1)
                    def _():
                        ring_copy(a, way, 1 - way).start()

        def one(i, c):
            with jax.named_scope("dispatch"):
                dispatch(a + i * (n_sp - 2 * a), jnp.maximum(2 * a - 1, 0) + i)
            return c

        count = jnp.where(jnp.logical_or(a == 0, a == half), 1, 2)
        lax.fori_loop(0, count, one, 0)

    def run_expert(p, count):
        with jax.named_scope("disp_wait"):
            for i in range(count):
                for kind in range(2):
                    for b in range(wide):

                        @pl.when(jnp.logical_not(is_own(kind, b)))
                        def _():
                            disp_arrival(kind, p + i, b).wait_recv()

        span = pl.ds(pl.multiple_of(p * 2 * batch, 2 * batch), count * 2 * batch)
        with jax.named_scope("ffn"):
            results[span] = ffn(arrived[span], eg, eu, ed).astype(jnp.bfloat16)

    def give_back(p):
        for kind in range(2):
            for b in range(wide):
                own = is_own(kind, b)

                @pl.when(jnp.logical_not(own))
                def _():
                    ret_copy(kind, p, b).start()

                @pl.when(own)
                def _():
                    returned[p, slots(member)] = results[row_of(kind, p, b)]

    def combine(d, p):
        with jax.named_scope("ret_wait"):
            for j in range(1, n_tp):
                ret_arrival(p, j).wait_recv()
        meta = metas[d]
        mix = jnp.zeros((group, rows), jnp.float32)
        for k in range(top):
            mix = jnp.where(matches(meta, k), meta[top + k : top + k + 1, :], mix)
        return lax.dot_general(
            mix.astype(jnp.bfloat16), returned[p], (((0,), (0,)), ((), ())),
            preferred_element_type=jnp.float32,
        )

    def reduce_start():
        for way in range(2):
            for h in range(2):
                for s in range(half - 1 if h != way else half):
                    ring_copy(s, way, h).wait_send()
        gathered[half] = combine(half, n_sp - 1).astype(jnp.bfloat16)
        red_copy(half, 0, 0).start()
        red_copy(half, 1, 1).start()

    def reduce_step(s):
        ways = ((s, 2 * s - 1, left_in), (n_sp - s, 2 * s, right_in))
        for way, (d, p, _) in enumerate(ways):
            parts[way] = combine(d, p)
        for order in range(2):
            for way, (d, _, buf_in) in enumerate(ways):
                h = 1 - way if order == 0 else way
                at = slice(h * mid, (h + 1) * mid)

                def add():
                    with jax.named_scope("red_wait"):
                        red_copy(s + 1, way, h).wait_recv()
                    gathered[d, at] = (parts[way, at] + buf_in[s, at].astype(jnp.float32)).astype(
                        jnp.bfloat16
                    )

                if order == 0:
                    pl.when(s < half - 1)(add)

                    @pl.when(s == half - 1)
                    def _():
                        gathered[d, at] = parts[way, at].astype(jnp.bfloat16)
                else:
                    add()
                red_copy(s, way, h).start()

    def finish():
        total[...] += combine(0, 0)
        for order in range(2):
            for way in range(2):
                with jax.named_scope("red_wait_last"):
                    red_copy(1, way, 1 - way if order == 0 else way).wait_recv()
        result[...] = (
            total[...] + left_in[0].astype(jnp.float32) + right_in[0].astype(jnp.float32)
        ).astype(result.dtype)

    def step(k, carry):
        @pl.when(k <= half)
        def _():
            gather_action(k)

        @pl.when(k == 1)
        def _():
            for copy in weights[7:]:
                copy.wait()

        @pl.when(jnp.logical_and(k > 1, k <= half))
        def _():
            run_expert(2 * k - 3, 2)

        @pl.when(jnp.logical_or(k == 1, k == half))
        def _():
            run_expert(jnp.where(k == 1, 0, n_sp - 1), 1)

        @pl.when(k == half)
        def _():
            give_back(n_sp - 1)
            for copy in weights[4:7]:
                copy.wait()
            with jax.named_scope("shared"):
                total[...] += ffn(gathered[0], sg, su, sd)

        @pl.when(k == half + 1)
        def _():
            reduce_start()

        @pl.when(k > half + 1)
        def _():
            reduce_step(2 * half + 1 - k)

        @pl.when(jnp.logical_and(k >= half, k <= 2 * half - 2))
        def _():
            give_back(4 * half - 3 - 2 * k)
            give_back(4 * half - 2 - 2 * k)

        @pl.when(k == 2 * half - 2)
        def _():
            give_back(0)

        return carry

    lax.fori_loop(0, 2 * half + 1, step, 0)
    finish()
    write = pltpu.make_async_copy(result, out, out_sem)
    write.start()

    for s in range(half):
        meta_copy(s, 0).wait_send()
        if s < half - 1:
            meta_copy(s, 1).wait_send()
    for t in range(n_tp):

        @pl.when(tp != t)
        def _():
            for i in range(2):
                conv_copy(t, i).wait_send()

    for way in range(2):
        halo_copy(way).wait_send()
        red_copy(half, way, way).wait_send()
        for s in range(1, half):
            for h in range(2):
                red_copy(s, way, h).wait_send()

    def drain(p, c):
        for j in range(1, n_tp):
            disp_copy(p, j).wait_send()
        for kind in range(2):
            for b in range(wide):

                @pl.when(jnp.logical_not(is_own(kind, b)))
                def _():
                    ret_copy(kind, p, b).wait_send()

        return c

    lax.fori_loop(0, n_sp, drain, 0)
    write.wait()


def body(
    out_gate,
    in_gate,
    conv_values,
    conv_taps,
    mix_gain,
    out_proj,
    residual,
    ffn_gain,
    routes,
    route_weights,
    shared_gate,
    shared_up,
    shared_down,
    expert_gate,
    expert_up,
    expert_down,
):
    n_sp, n_tp = lax.axis_size("sp"), lax.axis_size("tp")
    length, channels = in_gate.shape
    rows, width = residual.shape
    top = routes.shape[1]
    cap = max(2, 4 * rows * top // (3 * n_sp * n_tp))
    hidden, shared_hidden = expert_gate.shape[-1], shared_gate.shape[-1]
    half = n_sp // 2
    group = n_tp * cap
    wide = n_tp // 2
    bf, f32 = jnp.bfloat16, jnp.float32
    anywhere = pl.BlockSpec(memory_space=pl.ANY)
    dma = pltpu.SemaphoreType.DMA
    return pl.pallas_call(
        functools.partial(experts_kernel, n_sp, n_tp, cap, top),
        out_shape=jax.ShapeDtypeStruct((rows, width), bf),
        in_specs=[anywhere] * 16,
        out_specs=anywhere,
        scratch_shapes=[
            pltpu.VMEM(conv_taps.shape, f32),
            pltpu.VMEM(mix_gain.shape, f32),
            pltpu.VMEM((rows, width), bf),
            pltpu.VMEM((1, width), f32),
            pltpu.VMEM((top, rows), jnp.int32),
            pltpu.VMEM((top, rows), f32),
            pltpu.VMEM((rows, width), bf),
            pltpu.VMEM((length, channels), bf),
            pltpu.VMEM((length + HALO, channels), bf),
            pltpu.VMEM((length + HALO, channels), bf),
            pltpu.VMEM((n_tp, rows, channels), bf),
            pltpu.VMEM((n_tp, rows, channels), bf),
            pltpu.VMEM((n_sp, rows, width), bf),
            pltpu.VMEM((n_sp, META_ROWS, rows), f32),
            pltpu.VMEM((n_sp, group, width), bf),
            pltpu.VMEM((n_sp * group, width), bf),
            pltpu.VMEM((n_sp * group, width), bf),
            pltpu.VMEM((n_sp, group, width), bf),
            pltpu.VMEM((half, rows, width), bf),
            pltpu.VMEM((half, rows, width), bf),
            pltpu.VMEM((rows, width), f32),
            pltpu.VMEM((2, rows, width), f32),
            pltpu.VMEM((n_tp * channels, width), bf),
            pltpu.VMEM((width, hidden), bf),
            pltpu.VMEM((width, hidden), bf),
            pltpu.VMEM((hidden, width), bf),
            pltpu.VMEM((width, shared_hidden), bf),
            pltpu.VMEM((width, shared_hidden), bf),
            pltpu.VMEM((shared_hidden, width), bf),
            dma((10,)),
            dma((6,)),
            dma(()),
            dma((2,)),
            dma((2,)),
            dma((n_tp, 2)),
            dma((n_tp, 2)),
            dma((2, half)),
            dma((2, half)),
            dma((2, half, 2)),
            dma((2, half, 2)),
            dma((n_sp, n_tp)),
            dma((2, n_sp, wide)),
            dma((2, n_sp, wide)),
            dma((n_sp, n_tp)),
            dma((2, half + 1, 2)),
            dma((2, half + 1, 2)),
        ],
        compiler_params=pltpu.CompilerParams(
            collective_id=0, has_side_effects=True, vmem_limit_bytes=63 * 1024 * 1024
        ),
    )(
        out_gate, in_gate, conv_values, conv_taps, mix_gain,
        residual, ffn_gain.reshape(1, width), routes.T, route_weights.T,
        out_proj, expert_gate, expert_up, expert_down, shared_gate, shared_up, shared_down,
    )


def solution(mesh):
    in_specs = (
        P("sp", "tp"),
        P("sp", "tp"),
        P("sp", "tp"),
        P(None, "tp"),
        P(),
        P(),
        P(("sp", "tp"), None),
        P(),
        P(("sp", "tp"), None),
        P(("sp", "tp"), None),
        P(),
        P(),
        P(),
        P(("sp", "tp"), None, None),
        P(("sp", "tp"), None, None),
        P(("sp", "tp"), None, None),
    )
    out_specs = P(("sp", "tp"), None)
    return jax.shard_map(body, mesh=mesh, in_specs=in_specs, out_specs=out_specs, check_vma=False)
```

```python
import functools

import jax
import jax.numpy as jnp
from jax import lax
from jax.experimental import pallas as pl
from jax.experimental.pallas import tpu as pltpu
from jax.sharding import PartitionSpec as P

MESH = pl.DeviceIdType.MESH
META_ROWS = 16
HALO = 16


def ffn(x, gate, up, down):
    g = jnp.dot(x, gate[...], preferred_element_type=jnp.float32)
    u = jnp.dot(x, up[...], preferred_element_type=jnp.float32)
    h = (g / (1.0 + jnp.exp(-g)) * u).astype(jnp.bfloat16)
    return jnp.dot(h, down[...], preferred_element_type=jnp.float32)


def experts_kernel(
    n_sp, n_tp, cap, top,
    og_hbm, ig_hbm, cv_hbm, taps_hbm, mix_gain_hbm, residual_hbm, ffn_gain_hbm,
    routes_hbm, route_weights_hbm, op_hbm, eg_hbm, eu_hbm, ed_hbm, sg_hbm, su_hbm, sd_hbm,
    out,
    taps, mix_gain, residual, ffn_gain, routes, route_weights,
    og, ig, cv, conv_out, conv_in,
    gathered, metas, staged, arrived, results, returned,
    left_in, right_in, total, parts,
    op, eg, eu, ed, sg, su, sd,
    w_sem, small_sem, halo_send, halo_recv, conv_send, conv_recv,
    meta_send, meta_recv, ring_send, ring_recv,
    disp_send, disp_recv, ret_send, ret_recv, red_send, red_recv,
):
    sp = lax.axis_index("sp")
    tp = lax.axis_index("tp")
    half = n_sp // 2
    rows, width = total.shape
    length = og.shape[0]
    mid = width // 2
    group = n_tp * cap
    wide = n_tp // 2
    batch = wide * cap
    depth = n_sp // wide
    x, z = lax.rem(sp, wide), lax.div(sp, wide)
    y, core = lax.div(tp, 2), lax.rem(tp, 2)

    def across(kind):
        return y + kind * (x - y)

    def along(kind):
        return x + kind * (y - x)

    def device_at(kind, ring_index, member_index):
        zz, aa = lax.div(ring_index, wide), lax.rem(ring_index, wide)
        bb, cc = lax.div(member_index, 2), lax.rem(member_index, 2)
        return zz * wide + aa + kind * (bb - aa), (bb + kind * (aa - bb)) * 2 + cc

    ring = z * wide + along(core)
    member = across(core) * 2 + core

    def place_of(index):
        a, zz = lax.rem(index, wide), lax.div(index, wide)
        return a * depth + zz + lax.rem(a, 2) * (depth - 1 - 2 * zz)

    def index_of(place):
        a, zz = lax.div(place, depth), lax.rem(place, depth)
        return (zz + lax.rem(a, 2) * (depth - 1 - 2 * zz)) * wide + a

    place = place_of(ring)

    def ahead(distance):
        return device_at(core, index_of(lax.rem(place + distance, n_sp)), member)

    right, left = ahead(1), ahead(n_sp - 1)

    barrier = pltpu.get_barrier_semaphore()

    def greet(device):
        pl.semaphore_signal(barrier, inc=1, device_id=device, device_id_type=MESH)

    greet(right)
    greet(left)
    for j in range(1, n_tp):
        greet((sp, lax.rem(tp + j, n_tp)))
        greet(device_at(1, z * wide + y, lax.rem(x * 2 + core + j, n_tp)))
    greet((lax.rem(sp + 1, n_sp), tp))
    greet((lax.rem(sp + n_sp - 1, n_sp), tp))

    weights = [
        pltpu.make_async_copy(src, dst, w_sem.at[i])
        for i, (src, dst) in enumerate(
            ((ig_hbm, ig.at[pl.ds(HALO, length)]), (cv_hbm, cv.at[pl.ds(HALO, length)]),
             (og_hbm, og), (op_hbm, op), (sg_hbm, sg), (su_hbm, su), (sd_hbm, sd),
             (eg_hbm.at[0], eg), (eu_hbm.at[0], eu), (ed_hbm.at[0], ed))
        )
    ]
    smalls = [
        pltpu.make_async_copy(src, dst, small_sem.at[i])
        for i, (src, dst) in enumerate(
            ((taps_hbm, taps), (routes_hbm, routes), (route_weights_hbm, route_weights),
             (mix_gain_hbm, mix_gain), (ffn_gain_hbm, ffn_gain), (residual_hbm, residual))
        )
    ]
    for copy in weights[:2] + smalls[:1] + weights[2:3] + smalls[1:] + weights[3:4]:
        copy.start()

    def remote(src, dst, send, recv, device):
        return pltpu.make_async_remote_copy(
            src_ref=src, dst_ref=dst, send_sem=send, recv_sem=recv,
            device_id=device, device_id_type=MESH,
        )

    def meta_copy(s, way):
        dst = metas.at[s + 1 if way == 0 else n_sp - s - 1]
        src = metas.at[s if way == 0 else turned(s)]
        device = right if way == 0 else left
        return remote(src, dst, meta_send, meta_recv.at[way, s], device)

    def part_of(h):
        return pl.ds(h * mid, mid)

    def turned(s):
        return lax.rem(n_sp - s, n_sp)

    def ring_copy(s, way, h):
        dst = gathered.at[s + 1 if way == 0 else n_sp - s - 1, :, part_of(h)]
        src = gathered.at[s if way == 0 else turned(s), :, part_of(h)]
        device = right if way == 0 else left
        return remote(src, dst, ring_send, ring_recv.at[way, s, h], device)

    def slots(index):
        return pl.ds(pl.multiple_of(index * cap, cap), cap)

    def row_of(kind, p, b):
        return slots((p * 2 + kind) * wide + b)

    def disp_copy(p, j, h):
        to = lax.rem(member + j, n_tp)
        return remote(
            staged.at[p, slots(to), part_of(h)],
            arrived.at[row_of(core, p, across(core)), part_of(h)],
            disp_send, disp_recv.at[p],
            device_at(core, ring, to),
        )

    def is_own(kind, b):
        return jnp.logical_and(core == kind, across(kind) == b)

    def holder(kind, b):
        return device_at(kind, z * wide + along(kind), b * 2 + kind)

    others = pl.ds(0, (n_tp - 1) * cap)
    blocks = pl.ds(0, n_sp * (n_tp - 1) // n_tp)
    peers = pl.ds(0, n_sp - 1)

    def disp_arrival(p):
        return remote(
            staged.at[p, others], arrived.at[others], disp_send, disp_recv.at[p], right
        )

    def ret_copy(kind, p, b, h):
        me = across(kind) * 2 + core
        return remote(
            results.at[row_of(kind, p, b), part_of(h)], returned.at[p, slots(me), part_of(h)],
            ret_send, ret_recv.at[p, h], holder(kind, b),
        )

    def ret_arrival(p, h):
        return remote(
            results.at[others, part_of(h)], returned.at[p, others, part_of(h)],
            ret_send, ret_recv.at[p, h], right,
        )

    def red_copy(s, way, h):
        device = left if way == 0 else right
        src = gathered.at[s if way == 0 else n_sp - s, :, part_of(h)]
        dst = (left_in if way == 0 else right_in).at[s - 1, :, part_of(h)]
        return remote(src, dst, red_send, red_recv.at[way, s - 1, h], device)

    def halo_copy(i):
        buf = (ig, cv)[i]
        device = (lax.rem(sp + 1, n_sp), tp)
        return remote(
            buf.at[pl.ds(length, HALO)], buf.at[pl.ds(0, HALO)],
            halo_send, halo_recv.at[i], device,
        )

    pieces = (pl.ds(0, HALO), pl.ds(HALO, rows - HALO))

    def conv_copy(t, i):
        return remote(
            conv_out.at[t, pieces[i]], conv_in.at[tp, pieces[i]],
            conv_send, conv_recv.at[tp], (sp, t),
        )

    def conv_arrival(t):
        return remote(conv_out.at[t], conv_in.at[t], conv_send, conv_recv.at[t], (sp, t))

    taps_count = taps.shape[0]

    def convolve(t, first, count):
        span = pl.ds(t * rows + first, count + HALO)
        mixed = ig[span].astype(jnp.float32) * cv[span].astype(jnp.float32)
        if t == 0 and first == 0:
            blank = jnp.where(sp == 0, HALO, 0)
            at = lax.broadcasted_iota(jnp.int32, mixed.shape, 0)
            mixed = jnp.where(at >= blank, mixed, 0.0)
        base = HALO - (taps_count - 1)
        filtered = taps[0:1, :] * mixed[base : base + count]
        for o in range(1, taps_count):
            filtered = filtered + taps[o : o + 1, :] * mixed[base + o : base + o + count]
        gate = og[pl.ds(t * rows + first, count)].astype(jnp.float32)
        conv_out[t, pl.ds(first, count)] = (gate * filtered).astype(jnp.bfloat16)

    def send_conv(t, some):
        @pl.when(tp != t)
        def _():
            for i in some:
                conv_copy(t, i).start()

    owners = [t for t in range(2, n_tp, 2)] + [t for t in range(1, n_tp, 2)]
    for copy in weights[:3] + smalls[:1]:
        copy.wait()
    for t in owners:
        convolve(t, 0, rows)
    convolve(0, HALO, rows - HALO)
    with jax.named_scope("barrier"):
        pl.semaphore_wait(barrier, 2 + 2 * (n_tp - 1) + 2)
    halo_copy(0).start()
    halo_copy(1).start()
    for t in owners:
        send_conv(t, (1, 0))
    send_conv(0, (1,))
    for copy in weights[4:7]:
        copy.start()
    for copy in smalls[1:]:
        copy.wait()

    experts_total = n_sp * n_tp
    expert = lax.broadcasted_iota(jnp.int32, (experts_total, rows), 0)
    named = [routes[k : k + 1, :] == expert for k in range(top)]
    onehot = jnp.zeros((experts_total, rows), jnp.float32)
    for hit in named:
        onehot = jnp.where(hit, 1.0, onehot)
    earlier = lax.broadcasted_iota(jnp.int32, (rows, rows), 0) < lax.broadcasted_iota(
        jnp.int32, (rows, rows), 1
    )
    before = jnp.dot(
        onehot.astype(jnp.bfloat16),
        jnp.where(earlier, 1.0, 0.0).astype(jnp.bfloat16),
        preferred_element_type=jnp.float32,
    )

    def split(value, by):
        high = jnp.floor((value + 0.5) / by)
        return high, value - high * by

    rest, ec = split(expert.astype(jnp.float32), 2)
    rest, ey = split(rest, wide)
    ez, ex = split(rest, wide)
    turn = core.astype(jnp.float32)
    ea, eb = ex + turn * (ey - ex), ey + turn * (ex - ey)
    slot = before + ((ez * wide + ea) * n_tp + eb * 2 + ec) * cap
    metas[0] = jnp.zeros(metas.shape[1:], jnp.float32)
    for k in range(top):
        metas[0, k : k + 1, :] = jnp.sum(jnp.where(named[k], slot, 0.0), axis=0, keepdims=True)
    weight = route_weights[...]
    metas[0, top : 2 * top, :] = weight / jnp.sum(weight, axis=0, keepdims=True) * 2.5

    with jax.named_scope("halo_wait"):
        halo_copy(0).wait_recv()
        halo_copy(1).wait_recv()
    convolve(0, 0, HALO)
    send_conv(0, (0,))
    weights[3].wait()
    for copy in weights[7:]:
        copy.start()

    squares = jnp.zeros((rows, 1), jnp.float32)
    product = jnp.zeros((rows, width), jnp.float32)
    part_width = conv_in.shape[2]
    gains = mix_gain[...].reshape(1, n_tp * part_width)
    sources = [tp, tp + 1 - 2 * core]
    for i in range(1, wide):
        other = lax.rem(y + i, wide) * 2
        sources += [other, other + 1]
    for i, t in enumerate(sources):
        if i == 0:
            value = conv_out[t].astype(jnp.float32)
        else:
            with jax.named_scope("conv_wait"):
                conv_arrival(t).wait_recv()
            value = conv_in[t].astype(jnp.float32)
        gain = gains[:, :part_width]
        for k in range(1, n_tp):
            gain = jnp.where(t == k, gains[:, k * part_width : (k + 1) * part_width], gain)
        squares = squares + jnp.sum(value * value, axis=1, keepdims=True)
        product = product + jnp.dot(
            (value * gain).astype(jnp.bfloat16),
            op[pl.ds(pl.multiple_of(t * part_width, part_width), part_width), :],
            preferred_element_type=jnp.float32,
        )
    inverse = lax.rsqrt(squares / (n_tp * part_width) + 1e-06)
    stream = residual[...].astype(jnp.float32) + product * inverse
    power = jnp.mean(stream * stream, axis=1, keepdims=True)
    gathered[0] = (stream * lax.rsqrt(power + 1e-06) * ffn_gain[...]).astype(jnp.bfloat16)
    total[...] = stream

    first_slot = (ring * group).astype(jnp.float32)

    def matches(meta, k):
        at = lax.broadcasted_iota(jnp.int32, (group, rows), 0).astype(jnp.float32) + first_slot
        return at == meta[k : k + 1, :]

    def dispatch(d, p, h):
        meta = metas[d]
        pick = jnp.zeros((group, rows), jnp.float32)
        for k in range(top):
            pick = jnp.where(matches(meta, k), 1.0, pick)
        staged[p, :, part_of(h)] = jnp.dot(
            pick.astype(jnp.bfloat16), gathered[d, :, part_of(h)],
            preferred_element_type=jnp.float32,
        ).astype(jnp.bfloat16)
        for j in range(1, n_tp):
            disp_copy(p, j, h).start()
        arrived[row_of(core, p, across(core)), part_of(h)] = staged[p, slots(member), part_of(h)]

    def gather_action(a):
        @pl.when(a == 0)
        def _():
            for h in range(2):
                for way in range(2):
                    if h == 0:
                        meta_copy(0, way).start()
                    ring_copy(0, way, way if h == 0 else 1 - way).start()

        @pl.when(a > 0)
        def _():
            meta_copy(a - 1, 0).wait_recv()

            @pl.when(a < half)
            def _():
                meta_copy(a, 0).start()
                meta_copy(a - 1, 1).wait_recv()

            @pl.when(a < half - 1)
            def _():
                meta_copy(a, 1).start()

            for way in range(2):
                with jax.named_scope("ring_wait"):
                    ring_copy(a - 1, way, way).wait_recv()

                @pl.when(a < half)
                def _():
                    ring_copy(a, way, way).start()

        alone = jnp.logical_or(a == 0, a == half)
        low = jnp.maximum(2 * a - 1, 0)
        ways = ((a, low), (turned(a), jnp.where(alone, low, 2 * a)))
        for way, (d, p) in enumerate(ways):
            with jax.named_scope("dispatch"):
                dispatch(d, p, way)

        @pl.when(jnp.logical_not(alone))
        def _():
            for way in range(2):
                with jax.named_scope("ring_wait"):
                    ring_copy(a - 1, way, 1 - way).wait_recv()

                @pl.when(a < half - 1)
                def _():
                    ring_copy(a, way, 1 - way).start()

            for way, (d, p) in enumerate(ways):
                with jax.named_scope("dispatch"):
                    dispatch(d, p, 1 - way)

    def run_expert(p, count):
        with jax.named_scope("disp_wait"):
            for i in range(count):
                disp_arrival(p + i).wait_recv()

        span = pl.ds(pl.multiple_of(p * 2 * batch, 2 * batch), count * 2 * batch)
        with jax.named_scope("ffn"):
            results[span] = ffn(arrived[span], eg, eu, ed).astype(jnp.bfloat16)

    def give_back(p, h):
        for kind in range(2):
            for b in range(wide):
                own = is_own(kind, b)

                @pl.when(jnp.logical_not(own))
                def _():
                    ret_copy(kind, p, b, h).start()

                @pl.when(own)
                def _():
                    returned[p, slots(member), part_of(h)] = results[
                        row_of(kind, p, b), part_of(h)
                    ]

    def combine(d, p, h):
        with jax.named_scope("ret_wait"):
            ret_arrival(p, h).wait_recv()
        meta = metas[d]
        mix = jnp.zeros((group, rows), jnp.float32)
        for k in range(top):
            mix = jnp.where(matches(meta, k), meta[top + k : top + k + 1, :], mix)
        return lax.dot_general(
            mix.astype(jnp.bfloat16), returned[p, :, part_of(h)], (((0,), (0,)), ((), ())),
            preferred_element_type=jnp.float32,
        )

    def reduce_part(s, late, first):
        for way, buf_in in enumerate((left_in, right_in)):
            h = way if late else 1 - way
            d = s if way == 0 else n_sp - s
            p = jnp.minimum(2 * s - 1 + way, n_sp - 1)
            parts[way] = combine(d, p, h)
        for way, buf_in in enumerate((left_in, right_in)):
            h = way if late else 1 - way
            d = s if way == 0 else n_sp - s

            @pl.when(jnp.logical_not(first))
            def _():
                with jax.named_scope("red_wait"):
                    red_copy(s + 1, way, h).wait_recv()
                gathered[d, :, part_of(h)] = (
                    parts[way] + buf_in[s, :, part_of(h)].astype(jnp.float32)
                ).astype(jnp.bfloat16)

            @pl.when(first)
            def _():
                gathered[d, :, part_of(h)] = parts[way].astype(jnp.bfloat16)

            red_copy(s, way, h).start()

    def gather_step(k, carry):
        gather_action(k)

        @pl.when(k == 0)
        def _():
            for copy in weights[4:7]:
                copy.wait()
            with jax.named_scope("shared"):
                total[...] += ffn(gathered[0], sg, su, sd)
            for copy in weights[7:]:
                copy.wait()

        @pl.when(k > 1)
        def _():
            run_expert(2 * k - 3, 2)

        @pl.when(k == half - 1)
        def _():
            give_back(0, 0)
            give_back(0, 1)

        @pl.when(k == half)
        def _():
            give_back(n_sp - 3, 1)
            give_back(n_sp - 2, 0)

        @pl.when(jnp.logical_or(k == 1, k == half))
        def _():
            run_expert(jnp.where(k == 1, 0, n_sp - 1), 1)

        return carry

    lax.fori_loop(0, half + 1, gather_step, 0)
    for h in range(2):
        give_back(n_sp - 1, h)
    remote(gathered.at[peers], gathered.at[peers], ring_send, ring_recv.at[0, 0, 0], right).wait_send()

    def reduce_step(i, carry):
        @pl.when(i < half - 1)
        def _():
            reduce_part(half - 1 - i, False, i == 0)

        s = half - 1 - i

        @pl.when(s > 1)
        def _():
            give_back(2 * s - 3, 1)
            give_back(2 * s - 2, 0)

        @pl.when(s > 0)
        def _():
            give_back(2 * s - 1, 0)
            give_back(2 * s, 1)

        reduce_part(half - i, True, i == 0)
        return carry

    lax.fori_loop(0, half, reduce_step, 0)
    for h in range(2):
        total[:, part_of(h)] += combine(0, 0, h)
    with jax.named_scope("drain"):
        for buf, part, sem in (
            (metas, peers, meta_send), (conv_out, pl.ds(0, n_tp - 1), conv_send),
            (conv_out, (0, pl.ds(0, 2 * HALO)), halo_send), (staged, blocks, disp_send),
            (results, pl.ds(0, n_sp * (n_tp - 1) * cap), ret_send),
        ):
            remote(buf.at[part], buf.at[part], sem, halo_recv.at[0], right).wait_send()
    with jax.named_scope("red_wait_last"):
        for way in range(2):
            for h in range(2):
                red_copy(1, way, h).wait_recv()
    out[...] = (
        total[...] + left_in[0].astype(jnp.float32) + right_in[0].astype(jnp.float32)
    ).astype(out.dtype)

    with jax.named_scope("drain2"):
        remote(gathered.at[peers], gathered.at[peers], red_send, halo_recv.at[0], right).wait_send()


def body(
    out_gate,
    in_gate,
    conv_values,
    conv_taps,
    mix_gain,
    out_proj,
    residual,
    ffn_gain,
    routes,
    route_weights,
    shared_gate,
    shared_up,
    shared_down,
    expert_gate,
    expert_up,
    expert_down,
):
    n_sp, n_tp = lax.axis_size("sp"), lax.axis_size("tp")
    length, channels = in_gate.shape
    rows, width = residual.shape
    top = routes.shape[1]
    cap = max(2, 4 * rows * top // (3 * n_sp * n_tp))
    hidden, shared_hidden = expert_gate.shape[-1], shared_gate.shape[-1]
    half = n_sp // 2
    group = n_tp * cap
    wide = n_tp // 2
    bf, f32 = jnp.bfloat16, jnp.float32
    dma = pltpu.SemaphoreType.DMA
    return pl.pallas_call(
        functools.partial(experts_kernel, n_sp, n_tp, cap, top),
        out_shape=pltpu.VMEM((rows, width), bf),
        in_specs=[pl.BlockSpec(memory_space=pltpu.HBM)] * 16,
        out_specs=pl.BlockSpec(memory_space=pltpu.VMEM),
        scratch_shapes=[
            pltpu.VMEM(conv_taps.shape, f32),
            pltpu.VMEM(mix_gain.shape, f32),
            pltpu.VMEM((rows, width), bf),
            pltpu.VMEM((1, width), f32),
            pltpu.VMEM((top, rows), jnp.int32),
            pltpu.VMEM((top, rows), f32),
            pltpu.VMEM((length, channels), bf),
            pltpu.VMEM((length + HALO, channels), bf),
            pltpu.VMEM((length + HALO, channels), bf),
            pltpu.VMEM((n_tp, rows, channels), bf),
            pltpu.VMEM((n_tp, rows, channels), bf),
            pltpu.VMEM((n_sp, rows, width), bf),
            pltpu.VMEM((n_sp, META_ROWS, rows), f32),
            pltpu.VMEM((n_sp, group, width), bf),
            pltpu.VMEM((n_sp * group, width), bf),
            pltpu.VMEM((n_sp * group, width), bf),
            pltpu.VMEM((n_sp, group, width), bf),
            pltpu.VMEM((half, rows, width), bf),
            pltpu.VMEM((half, rows, width), bf),
            pltpu.VMEM((rows, width), f32),
            pltpu.VMEM((2, rows, width // 2), f32),
            pltpu.VMEM((n_tp * channels, width), bf),
            pltpu.VMEM((width, hidden), bf),
            pltpu.VMEM((width, hidden), bf),
            pltpu.VMEM((hidden, width), bf),
            pltpu.VMEM((width, shared_hidden), bf),
            pltpu.VMEM((width, shared_hidden), bf),
            pltpu.VMEM((shared_hidden, width), bf),
            dma((10,)),
            dma((6,)),
            dma(()),
            dma((2,)),
            dma(()),
            dma((n_tp,)),
            dma(()),
            dma((2, half)),
            dma(()),
            dma((2, half, 2)),
            dma(()),
            dma((n_sp,)),
            dma(()),
            dma((n_sp, 2)),
            dma(()),
            dma((2, half, 2)),
        ],
        compiler_params=pltpu.CompilerParams(
            collective_id=0, has_side_effects=True, vmem_limit_bytes=58 * 1024 * 1024
        ),
    )(
        out_gate, in_gate, conv_values, conv_taps, mix_gain,
        residual, ffn_gain.reshape(1, width), routes.T, route_weights.T,
        out_proj, expert_gate, expert_up, expert_down, shared_gate, shared_up, shared_down,
    )


def solution(mesh):
    in_specs = (
        P("sp", "tp"),
        P("sp", "tp"),
        P("sp", "tp"),
        P(None, "tp"),
        P(),
        P(),
        P(("sp", "tp"), None),
        P(),
        P(("sp", "tp"), None),
        P(("sp", "tp"), None),
        P(),
        P(),
        P(),
        P(("sp", "tp"), None, None),
        P(("sp", "tp"), None, None),
        P(("sp", "tp"), None, None),
    )
    out_specs = P(("sp", "tp"), None)
    return jax.shard_map(body, mesh=mesh, in_specs=in_specs, out_specs=out_specs, check_vma=False)
```

```python
import functools

import jax
import jax.numpy as jnp
from jax import lax
from jax.experimental import pallas as pl
from jax.experimental.pallas import tpu as pltpu
from jax.sharding import PartitionSpec as P

MESH = pl.DeviceIdType.MESH
META_ROWS = 16
HALO = 16


def ffn(x, gate, up, down):
    g = jnp.dot(x, gate[...], preferred_element_type=jnp.float32)
    u = jnp.dot(x, up[...], preferred_element_type=jnp.float32)
    h = (g / (1.0 + jnp.exp(-g)) * u).astype(jnp.bfloat16)
    return jnp.dot(h, down[...], preferred_element_type=jnp.float32)


def experts_kernel(
    n_sp, n_tp, cap, top,
    og_hbm, ig_hbm, cv_hbm, taps_hbm, mix_gain_hbm, residual_hbm, ffn_gain_hbm,
    routes_hbm, route_weights_hbm, op_hbm, eg_hbm, eu_hbm, ed_hbm, sg_hbm, su_hbm, sd_hbm,
    out,
    taps, mix_gain, residual, ffn_gain, routes, route_weights,
    og, ig, cv, conv_out, conv_in,
    gathered, metas, staged, arrived, results, returned,
    left_in, right_in, total, parts,
    op, eg, eu, ed, sg, su, sd,
    w_sem, small_sem, halo_send, halo_recv, conv_send, conv_recv,
    meta_send, meta_recv, ring_send, ring_recv,
    disp_send, disp_recv, ret_send, ret_recv, red_send, red_recv,
):
    sp = lax.axis_index("sp")
    tp = lax.axis_index("tp")
    half = n_sp // 2
    rows, width = total.shape
    length = og.shape[0]
    mid = width // 2
    group = n_tp * cap
    wide = n_tp // 2
    batch = wide * cap
    depth = n_sp // wide
    x, z = lax.rem(sp, wide), lax.div(sp, wide)
    y, core = lax.div(tp, 2), lax.rem(tp, 2)

    def across(kind):
        return y + kind * (x - y)

    def along(kind):
        return x + kind * (y - x)

    def device_at(kind, ring_index, member_index):
        zz, aa = lax.div(ring_index, wide), lax.rem(ring_index, wide)
        bb, cc = lax.div(member_index, 2), lax.rem(member_index, 2)
        return zz * wide + aa + kind * (bb - aa), (bb + kind * (aa - bb)) * 2 + cc

    ring = z * wide + along(core)
    member = across(core) * 2 + core

    def place_of(index):
        a, zz = lax.rem(index, wide), lax.div(index, wide)
        return a * depth + zz + lax.rem(a, 2) * (depth - 1 - 2 * zz)

    def index_of(place):
        a, zz = lax.div(place, depth), lax.rem(place, depth)
        return (zz + lax.rem(a, 2) * (depth - 1 - 2 * zz)) * wide + a

    place = place_of(ring)

    def ahead(distance):
        return device_at(core, index_of(lax.rem(place + distance, n_sp)), member)

    right, left = ahead(1), ahead(n_sp - 1)

    barrier = pltpu.get_barrier_semaphore()

    def greet(device):
        pl.semaphore_signal(barrier, inc=1, device_id=device, device_id_type=MESH)

    greet(right)
    greet(left)
    for j in range(1, n_tp):
        greet((sp, lax.rem(tp + j, n_tp)))
        greet(device_at(1, z * wide + y, lax.rem(x * 2 + core + j, n_tp)))
    has_next, has_last = sp < n_sp - 1, sp > 0

    @pl.when(has_next)
    def _():
        greet((sp + 1, tp))

    @pl.when(has_last)
    def _():
        greet((sp - 1, tp))

    weights = [
        pltpu.make_async_copy(src, dst, w_sem.at[i])
        for i, (src, dst) in enumerate(
            ((ig_hbm, ig.at[pl.ds(HALO, length)]), (cv_hbm, cv.at[pl.ds(HALO, length)]),
             (og_hbm, og), (op_hbm, op), (sg_hbm, sg), (su_hbm, su), (sd_hbm, sd),
             (eg_hbm.at[0], eg), (eu_hbm.at[0], eu), (ed_hbm.at[0], ed))
        )
    ]
    smalls = [
        pltpu.make_async_copy(src, dst, small_sem.at[i])
        for i, (src, dst) in enumerate(
            ((taps_hbm, taps), (routes_hbm, routes), (route_weights_hbm, route_weights),
             (mix_gain_hbm, mix_gain), (ffn_gain_hbm, ffn_gain), (residual_hbm, residual))
        )
    ]
    for copy in weights[:2] + smalls[:1] + weights[2:3] + smalls[1:] + weights[3:4]:
        copy.start()

    def remote(src, dst, send, recv, device):
        return pltpu.make_async_remote_copy(
            src_ref=src, dst_ref=dst, send_sem=send, recv_sem=recv,
            device_id=device, device_id_type=MESH,
        )

    def meta_copy(s, way):
        dst = metas.at[s + 1 if way == 0 else n_sp - s - 1]
        src = metas.at[s if way == 0 else turned(s)]
        device = right if way == 0 else left
        return remote(src, dst, meta_send, meta_recv.at[way, s], device)

    def part_of(h):
        return pl.ds(h * mid, mid)

    def turned(s):
        return lax.rem(n_sp - s, n_sp)

    def ring_copy(s, way, h):
        dst = gathered.at[s + 1 if way == 0 else n_sp - s - 1, :, part_of(h)]
        src = gathered.at[s if way == 0 else turned(s), :, part_of(h)]
        device = right if way == 0 else left
        return remote(src, dst, ring_send, ring_recv.at[way, s, h], device)

    def slots(index):
        return pl.ds(pl.multiple_of(index * cap, cap), cap)

    def row_of(kind, p, b):
        return slots((p * 2 + kind) * wide + b)

    def disp_copy(p, j, h):
        to = lax.rem(member + j, n_tp)
        return remote(
            staged.at[p, slots(to), part_of(h)],
            arrived.at[row_of(core, p, across(core)), part_of(h)],
            disp_send, disp_recv.at[p],
            device_at(core, ring, to),
        )

    def is_own(kind, b):
        return jnp.logical_and(core == kind, across(kind) == b)

    def holder(kind, b):
        return device_at(kind, z * wide + along(kind), b * 2 + kind)

    others = pl.ds(0, (n_tp - 1) * cap)
    blocks = pl.ds(0, n_sp * (n_tp - 1) // n_tp)
    peers = pl.ds(0, n_sp - 1)

    def disp_arrival(p):
        return remote(
            staged.at[p, others], arrived.at[others], disp_send, disp_recv.at[p], right
        )

    def ret_copy(kind, p, b, h):
        me = across(kind) * 2 + core
        return remote(
            results.at[row_of(kind, p, b), part_of(h)], returned.at[p, slots(me), part_of(h)],
            ret_send, ret_recv.at[p, h], holder(kind, b),
        )

    def ret_arrival(p, h):
        return remote(
            results.at[others, part_of(h)], returned.at[p, others, part_of(h)],
            ret_send, ret_recv.at[p, h], right,
        )

    def red_copy(s, way, h):
        device = left if way == 0 else right
        src = gathered.at[s if way == 0 else n_sp - s, :, part_of(h)]
        dst = (left_in if way == 0 else right_in).at[s - 1, :, part_of(h)]
        return remote(src, dst, red_send, red_recv.at[way, s - 1, h], device)

    def halo_copy(i):
        buf = (ig, cv)[i]
        device = (lax.rem(sp + 1, n_sp), tp)
        return remote(
            buf.at[pl.ds(length, HALO)], buf.at[pl.ds(0, HALO)],
            halo_send, halo_recv.at[i], device,
        )

    pieces = (pl.ds(0, HALO), pl.ds(HALO, rows - HALO))

    def conv_copy(t, i):
        return remote(
            conv_out.at[t, pieces[i]], conv_in.at[tp, pieces[i]],
            conv_send, conv_recv.at[tp], (sp, t),
        )

    def conv_arrival(t):
        return remote(conv_out.at[t], conv_in.at[t], conv_send, conv_recv.at[t], (sp, t))

    taps_count = taps.shape[0]

    def convolve(t, first, count):
        span = pl.ds(t * rows + first, count + HALO)
        mixed = ig[span].astype(jnp.float32) * cv[span].astype(jnp.float32)
        base = HALO - (taps_count - 1)
        filtered = taps[0:1, :] * mixed[base : base + count]
        for o in range(1, taps_count):
            filtered = filtered + taps[o : o + 1, :] * mixed[base + o : base + o + count]
        gate = og[pl.ds(t * rows + first, count)].astype(jnp.float32)
        conv_out[t, pl.ds(first, count)] = (gate * filtered).astype(jnp.bfloat16)

    def send_conv(t, some):
        @pl.when(tp != t)
        def _():
            for i in some:
                conv_copy(t, i).start()

    owners = [t for t in range(2, n_tp, 2)] + [t for t in range(1, n_tp, 2)]
    for copy in weights[:3] + smalls[:1]:
        copy.wait()
    for t in owners:
        convolve(t, 0, rows)
    convolve(0, HALO, rows - HALO)
    with jax.named_scope("barrier"):
        near = has_next.astype(jnp.int32) + has_last.astype(jnp.int32)
        pl.semaphore_wait(barrier, 2 + 2 * (n_tp - 1) + near)

    @pl.when(has_next)
    def _():
        halo_copy(0).start()
        halo_copy(1).start()

    for t in owners:
        send_conv(t, (1, 0))
    send_conv(0, (1,))
    for copy in weights[4:7]:
        copy.start()
    for copy in smalls[1:]:
        copy.wait()

    experts_total = n_sp * n_tp
    expert = lax.broadcasted_iota(jnp.int32, (experts_total, rows), 0)
    named = [routes[k : k + 1, :] == expert for k in range(top)]
    onehot = jnp.zeros((experts_total, rows), jnp.float32)
    for hit in named:
        onehot = jnp.where(hit, 1.0, onehot)
    earlier = lax.broadcasted_iota(jnp.int32, (rows, rows), 0) < lax.broadcasted_iota(
        jnp.int32, (rows, rows), 1
    )
    before = jnp.dot(
        onehot.astype(jnp.bfloat16),
        jnp.where(earlier, 1.0, 0.0).astype(jnp.bfloat16),
        preferred_element_type=jnp.float32,
    )

    def split(value, by):
        high = jnp.floor((value + 0.5) / by)
        return high, value - high * by

    rest, ec = split(expert.astype(jnp.float32), 2)
    rest, ey = split(rest, wide)
    ez, ex = split(rest, wide)
    turn = core.astype(jnp.float32)
    ea, eb = ex + turn * (ey - ex), ey + turn * (ex - ey)
    slot = before + ((ez * wide + ea) * n_tp + eb * 2 + ec) * cap
    metas[0] = jnp.zeros(metas.shape[1:], jnp.float32)
    for k in range(top):
        metas[0, k : k + 1, :] = jnp.sum(jnp.where(named[k], slot, 0.0), axis=0, keepdims=True)
    weight = route_weights[...]
    metas[0, top : 2 * top, :] = weight / jnp.sum(weight, axis=0, keepdims=True) * 2.5

    @pl.when(has_last)
    def _():
        with jax.named_scope("halo_wait"):
            halo_copy(0).wait_recv()
            halo_copy(1).wait_recv()

    @pl.when(jnp.logical_not(has_last))
    def _():
        for buf in (ig, cv):
            buf[pl.ds(0, HALO)] = jnp.zeros((HALO, buf.shape[1]), buf.dtype)

    convolve(0, 0, HALO)
    send_conv(0, (0,))
    weights[3].wait()
    for copy in weights[7:]:
        copy.start()

    squares = jnp.zeros((rows, 1), jnp.float32)
    product = jnp.zeros((rows, width), jnp.float32)
    part_width = conv_in.shape[2]
    gains = mix_gain[...].reshape(1, n_tp * part_width)
    sources = [tp, tp + 1 - 2 * core]
    for i in range(1, wide):
        other = lax.rem(y + i, wide) * 2
        sources += [other, other + 1]
    for i, t in enumerate(sources):
        if i == 0:
            value = conv_out[t].astype(jnp.float32)
        else:
            with jax.named_scope("conv_wait"):
                conv_arrival(t).wait_recv()
            value = conv_in[t].astype(jnp.float32)
        gain = gains[:, :part_width]
        for k in range(1, n_tp):
            gain = jnp.where(t == k, gains[:, k * part_width : (k + 1) * part_width], gain)
        squares = squares + jnp.sum(value * value, axis=1, keepdims=True)
        product = product + jnp.dot(
            (value * gain).astype(jnp.bfloat16),
            op[pl.ds(pl.multiple_of(t * part_width, part_width), part_width), :],
            preferred_element_type=jnp.float32,
        )
    inverse = lax.rsqrt(squares / (n_tp * part_width) + 1e-06)
    stream = residual[...].astype(jnp.float32) + product * inverse
    power = jnp.mean(stream * stream, axis=1, keepdims=True)
    gathered[0] = (stream * lax.rsqrt(power + 1e-06) * ffn_gain[...]).astype(jnp.bfloat16)
    total[...] = stream

    first_slot = (ring * group).astype(jnp.float32)

    def matches(meta, k):
        at = lax.broadcasted_iota(jnp.int32, (group, rows), 0).astype(jnp.float32) + first_slot
        return at == meta[k : k + 1, :]

    def dispatch(d, p, h):
        meta = metas[d]
        pick = jnp.zeros((group, rows), jnp.float32)
        for k in range(top):
            pick = jnp.where(matches(meta, k), 1.0, pick)
        staged[p, :, part_of(h)] = jnp.dot(
            pick.astype(jnp.bfloat16), gathered[d, :, part_of(h)],
            preferred_element_type=jnp.float32,
        ).astype(jnp.bfloat16)
        for j in range(1, n_tp):
            disp_copy(p, j, h).start()
        arrived[row_of(core, p, across(core)), part_of(h)] = staged[p, slots(member), part_of(h)]

    def gather_action(a):
        @pl.when(a == 0)
        def _():
            for h in range(2):
                for way in range(2):
                    if h == 0:
                        meta_copy(0, way).start()
                    ring_copy(0, way, way if h == 0 else 1 - way).start()

        @pl.when(a > 0)
        def _():
            meta_copy(a - 1, 0).wait_recv()

            @pl.when(a < half)
            def _():
                meta_copy(a, 0).start()
                meta_copy(a - 1, 1).wait_recv()

            @pl.when(a < half - 1)
            def _():
                meta_copy(a, 1).start()

            for way in range(2):
                with jax.named_scope("ring_wait"):
                    ring_copy(a - 1, way, way).wait_recv()

                @pl.when(a < half)
                def _():
                    ring_copy(a, way, way).start()

        alone = jnp.logical_or(a == 0, a == half)
        low = jnp.maximum(2 * a - 1, 0)
        ways = ((a, low), (turned(a), jnp.where(alone, low, 2 * a)))
        for way, (d, p) in enumerate(ways):
            with jax.named_scope("dispatch"):
                dispatch(d, p, way)

        @pl.when(jnp.logical_not(alone))
        def _():
            for way in range(2):
                with jax.named_scope("ring_wait"):
                    ring_copy(a - 1, way, 1 - way).wait_recv()

                @pl.when(a < half - 1)
                def _():
                    ring_copy(a, way, 1 - way).start()

            for way, (d, p) in enumerate(ways):
                with jax.named_scope("dispatch"):
                    dispatch(d, p, 1 - way)

    def run_expert(p, count):
        with jax.named_scope("disp_wait"):
            for i in range(count):
                disp_arrival(p + i).wait_recv()

        span = pl.ds(pl.multiple_of(p * 2 * batch, 2 * batch), count * 2 * batch)
        with jax.named_scope("ffn"):
            results[span] = ffn(arrived[span], eg, eu, ed).astype(jnp.bfloat16)

    def give_back(p, h):
        for kind in range(2):
            for b in range(wide):
                own = is_own(kind, b)

                @pl.when(jnp.logical_not(own))
                def _():
                    ret_copy(kind, p, b, h).start()

                @pl.when(own)
                def _():
                    returned[p, slots(member), part_of(h)] = results[
                        row_of(kind, p, b), part_of(h)
                    ]

    def combine(d, p, h):
        with jax.named_scope("ret_wait"):
            ret_arrival(p, h).wait_recv()
        meta = metas[d]
        mix = jnp.zeros((group, rows), jnp.float32)
        for k in range(top):
            mix = jnp.where(matches(meta, k), meta[top + k : top + k + 1, :], mix)
        return lax.dot_general(
            mix.astype(jnp.bfloat16), returned[p, :, part_of(h)], (((0,), (0,)), ((), ())),
            preferred_element_type=jnp.float32,
        )

    def reduce_part(s, late, first):
        for way in range(2):
            h = way if late else 1 - way
            d = s if way == 0 else n_sp - s
            parts[way] = combine(d, jnp.minimum(2 * s - 1 + way, n_sp - 1), h)

            @pl.when(first)
            def _():
                gathered[d, :, part_of(h)] = parts[way].astype(jnp.bfloat16)
                red_copy(s, way, h).start()

        @pl.when(jnp.logical_not(first))
        def _():
            for way, buf_in in enumerate((left_in, right_in)):
                h = way if late else 1 - way
                d = s if way == 0 else n_sp - s
                with jax.named_scope("red_wait"):
                    red_copy(s + 1, way, h).wait_recv()
                gathered[d, :, part_of(h)] = (
                    parts[way] + buf_in[s, :, part_of(h)].astype(jnp.float32)
                ).astype(jnp.bfloat16)
                red_copy(s, way, h).start()

    def gather_step(k, carry):
        gather_action(k)

        @pl.when(k == 0)
        def _():
            for copy in weights[4:7]:
                copy.wait()
            with jax.named_scope("shared"):
                total[...] += ffn(gathered[0], sg, su, sd)
            for copy in weights[7:]:
                copy.wait()

        @pl.when(k > 1)
        def _():
            run_expert(2 * k - 3, 2)

        @pl.when(k == half - 1)
        def _():
            give_back(n_sp - 5, 1)
            give_back(n_sp - 4, 0)

        @pl.when(k == half)
        def _():
            give_back(n_sp - 3, 1)
            give_back(n_sp - 2, 0)

        @pl.when(jnp.logical_or(k == 1, k == half))
        def _():
            run_expert(jnp.where(k == 1, 0, n_sp - 1), 1)

        return carry

    lax.fori_loop(0, half + 1, gather_step, 0)
    for h in range(2):
        give_back(n_sp - 1, h)
    remote(gathered.at[peers], gathered.at[peers], ring_send, ring_recv.at[0, 0, 0], right).wait_send()

    def reduce_step(i, carry):
        @pl.when(i < half - 1)
        def _():
            reduce_part(half - 1 - i, False, i == 0)

        s = half - 1 - i

        @pl.when(jnp.logical_and(s > 1, i > 0))
        def _():
            give_back(2 * s - 3, 1)
            give_back(2 * s - 2, 0)

        @pl.when(s > 0)
        def _():
            give_back(2 * s - 1, 0)
            give_back(2 * s, 1)

        @pl.when(s == 1)
        def _():
            give_back(0, 0)
            give_back(0, 1)

        reduce_part(half - i, True, i == 0)
        return carry

    lax.fori_loop(0, half, reduce_step, 0)
    for h in range(2):
        total[:, part_of(h)] += combine(0, 0, h)
    with jax.named_scope("drain"):
        for buf, part, sem in (
            (metas, peers, meta_send), (conv_out, pl.ds(0, n_tp - 1), conv_send),
            (staged, blocks, disp_send),
            (results, pl.ds(0, n_sp * (n_tp - 1) * cap), ret_send),
        ):
            remote(buf.at[part], buf.at[part], sem, halo_recv.at[0], right).wait_send()

        @pl.when(has_next)
        def _():
            both = conv_out.at[0, pl.ds(0, 2 * HALO)]
            remote(both, both, halo_send, halo_recv.at[0], right).wait_send()

    with jax.named_scope("red_wait_last"):
        for way in range(2):
            for h in range(2):
                red_copy(1, way, h).wait_recv()
    out[...] = (
        total[...] + left_in[0].astype(jnp.float32) + right_in[0].astype(jnp.float32)
    ).astype(out.dtype)

    with jax.named_scope("drain2"):
        remote(gathered.at[peers], gathered.at[peers], red_send, halo_recv.at[0], right).wait_send()


def body(
    out_gate,
    in_gate,
    conv_values,
    conv_taps,
    mix_gain,
    out_proj,
    residual,
    ffn_gain,
    routes,
    route_weights,
    shared_gate,
    shared_up,
    shared_down,
    expert_gate,
    expert_up,
    expert_down,
):
    n_sp, n_tp = lax.axis_size("sp"), lax.axis_size("tp")
    length, channels = in_gate.shape
    rows, width = residual.shape
    top = routes.shape[1]
    cap = max(2, 4 * rows * top // (3 * n_sp * n_tp))
    hidden, shared_hidden = expert_gate.shape[-1], shared_gate.shape[-1]
    half = n_sp // 2
    group = n_tp * cap
    wide = n_tp // 2
    bf, f32 = jnp.bfloat16, jnp.float32
    dma = pltpu.SemaphoreType.DMA
    return pl.pallas_call(
        functools.partial(experts_kernel, n_sp, n_tp, cap, top),
        out_shape=pltpu.VMEM((rows, width), bf),
        in_specs=[pl.BlockSpec(memory_space=pltpu.HBM)] * 16,
        out_specs=pl.BlockSpec(memory_space=pltpu.VMEM),
        scratch_shapes=[
            pltpu.VMEM(conv_taps.shape, f32),
            pltpu.VMEM(mix_gain.shape, f32),
            pltpu.VMEM((rows, width), bf),
            pltpu.VMEM((1, width), f32),
            pltpu.VMEM((top, rows), jnp.int32),
            pltpu.VMEM((top, rows), f32),
            pltpu.VMEM((length, channels), bf),
            pltpu.VMEM((length + HALO, channels), bf),
            pltpu.VMEM((length + HALO, channels), bf),
            pltpu.VMEM((n_tp, rows, channels), bf),
            pltpu.VMEM((n_tp, rows, channels), bf),
            pltpu.VMEM((n_sp, rows, width), bf),
            pltpu.VMEM((n_sp, META_ROWS, rows), f32),
            pltpu.VMEM((n_sp, group, width), bf),
            pltpu.VMEM((n_sp * group, width), bf),
            pltpu.VMEM((n_sp * group, width), bf),
            pltpu.VMEM((n_sp, group, width), bf),
            pltpu.VMEM((half, rows, width), bf),
            pltpu.VMEM((half, rows, width), bf),
            pltpu.VMEM((rows, width), f32),
            pltpu.VMEM((2, rows, width // 2), f32),
            pltpu.VMEM((n_tp * channels, width), bf),
            pltpu.VMEM((width, hidden), bf),
            pltpu.VMEM((width, hidden), bf),
            pltpu.VMEM((hidden, width), bf),
            pltpu.VMEM((width, shared_hidden), bf),
            pltpu.VMEM((width, shared_hidden), bf),
            pltpu.VMEM((shared_hidden, width), bf),
            dma((10,)),
            dma((6,)),
            dma(()),
            dma((2,)),
            dma(()),
            dma((n_tp,)),
            dma(()),
            dma((2, half)),
            dma(()),
            dma((2, half, 2)),
            dma(()),
            dma((n_sp,)),
            dma(()),
            dma((n_sp, 2)),
            dma(()),
            dma((2, half, 2)),
        ],
        compiler_params=pltpu.CompilerParams(
            collective_id=0, has_side_effects=True, vmem_limit_bytes=58 * 1024 * 1024
        ),
    )(
        out_gate, in_gate, conv_values, conv_taps, mix_gain,
        residual, ffn_gain.reshape(1, width), routes.T, route_weights.T,
        out_proj, expert_gate, expert_up, expert_down, shared_gate, shared_up, shared_down,
    )


def solution(mesh):
    in_specs = (
        P("sp", "tp"),
        P("sp", "tp"),
        P("sp", "tp"),
        P(None, "tp"),
        P(),
        P(),
        P(("sp", "tp"), None),
        P(),
        P(("sp", "tp"), None),
        P(("sp", "tp"), None),
        P(),
        P(),
        P(),
        P(("sp", "tp"), None, None),
        P(("sp", "tp"), None, None),
        P(("sp", "tp"), None, None),
    )
    out_specs = P(("sp", "tp"), None)
    return jax.shard_map(body, mesh=mesh, in_specs=in_specs, out_specs=out_specs, check_vma=False)
```

```python
import functools

import jax
import jax.numpy as jnp
from jax import lax
from jax.experimental import pallas as pl
from jax.experimental.pallas import tpu as pltpu
from jax.sharding import PartitionSpec as P

MESH = pl.DeviceIdType.MESH
META_ROWS = 16
HALO = 16


def ffn(x, gate, up, down):
    g = jnp.dot(x, gate[...], preferred_element_type=jnp.float32)
    u = jnp.dot(x, up[...], preferred_element_type=jnp.float32)
    h = (g / (1.0 + jnp.exp(-g)) * u).astype(jnp.bfloat16)
    return jnp.dot(h, down[...], preferred_element_type=jnp.float32)


def experts_kernel(
    n_sp, n_tp, cap, top,
    og_hbm, ig_hbm, cv_hbm, taps_hbm, mix_gain_hbm, residual_hbm, ffn_gain_hbm,
    routes_hbm, route_weights_hbm, op_hbm, eg_hbm, eu_hbm, ed_hbm, sg_hbm, su_hbm, sd_hbm,
    out,
    taps, mix_gain, residual, ffn_gain, routes, route_weights,
    og, ig, cv, conv_out, conv_in,
    gathered, metas, staged, arrived, results, returned,
    left_in, right_in, total, parts,
    op, eg, eu, ed, sg, su, sd,
    w_sem, small_sem, halo_send, halo_recv, conv_send, conv_recv,
    meta_send, meta_recv, ring_send, ring_recv,
    disp_send, disp_recv, ret_send, ret_recv, red_send, red_recv,
):
    sp = lax.axis_index("sp")
    tp = lax.axis_index("tp")
    half = n_sp // 2
    rows, width = total.shape
    length = og.shape[0]
    mid = width // 2
    group = n_tp * cap
    wide = n_tp // 2
    batch = wide * cap
    depth = n_sp // wide
    x, z = lax.rem(sp, wide), lax.div(sp, wide)
    y, core = lax.div(tp, 2), lax.rem(tp, 2)

    def across(kind):
        return y + kind * (x - y)

    def along(kind):
        return x + kind * (y - x)

    def device_at(kind, ring_index, member_index):
        zz, aa = lax.div(ring_index, wide), lax.rem(ring_index, wide)
        bb, cc = lax.div(member_index, 2), lax.rem(member_index, 2)
        return zz * wide + aa + kind * (bb - aa), (bb + kind * (aa - bb)) * 2 + cc

    ring = z * wide + along(core)
    member = across(core) * 2 + core

    def place_of(index):
        a, zz = lax.rem(index, wide), lax.div(index, wide)
        return a * depth + zz + lax.rem(a, 2) * (depth - 1 - 2 * zz)

    def index_of(place):
        a, zz = lax.div(place, depth), lax.rem(place, depth)
        return (zz + lax.rem(a, 2) * (depth - 1 - 2 * zz)) * wide + a

    place = place_of(ring)

    def ahead(distance):
        return device_at(core, index_of(lax.rem(place + distance, n_sp)), member)

    right, left = ahead(1), ahead(n_sp - 1)

    barrier = pltpu.get_barrier_semaphore()

    def greet(device):
        pl.semaphore_signal(barrier, inc=1, device_id=device, device_id_type=MESH)

    greet(right)
    greet(left)
    for j in range(1, n_tp):
        greet((sp, lax.rem(tp + j, n_tp)))
        greet(device_at(1, z * wide + y, lax.rem(x * 2 + core + j, n_tp)))
    has_next, has_last = sp < n_sp - 1, sp > 0

    @pl.when(has_next)
    def _():
        greet((sp + 1, tp))

    @pl.when(has_last)
    def _():
        greet((sp - 1, tp))

    weights = [
        pltpu.make_async_copy(src, dst, w_sem.at[i])
        for i, (src, dst) in enumerate(
            ((ig_hbm, ig.at[pl.ds(HALO, length)]), (cv_hbm, cv.at[pl.ds(HALO, length)]),
             (og_hbm, og), (op_hbm, op), (sg_hbm, sg), (su_hbm, su), (sd_hbm, sd),
             (eg_hbm.at[0], eg), (eu_hbm.at[0], eu), (ed_hbm.at[0], ed))
        )
    ]
    smalls = [
        pltpu.make_async_copy(src, dst, small_sem.at[i])
        for i, (src, dst) in enumerate(
            ((taps_hbm, taps), (routes_hbm, routes), (route_weights_hbm, route_weights),
             (mix_gain_hbm, mix_gain), (ffn_gain_hbm, ffn_gain), (residual_hbm, residual))
        )
    ]
    for copy in weights[:2] + smalls[:1] + weights[2:3] + smalls[1:] + weights[3:4]:
        copy.start()

    def remote(src, dst, send, recv, device):
        return pltpu.make_async_remote_copy(
            src_ref=src, dst_ref=dst, send_sem=send, recv_sem=recv,
            device_id=device, device_id_type=MESH,
        )

    def meta_copy(s, way):
        dst = metas.at[s + 1 if way == 0 else n_sp - s - 1]
        src = metas.at[s if way == 0 else turned(s)]
        device = right if way == 0 else left
        return remote(src, dst, meta_send, meta_recv.at[way, s], device)

    def part_of(h):
        return pl.ds(h * mid, mid)

    def turned(s):
        return lax.rem(n_sp - s, n_sp)

    def ring_copy(s, way, h):
        dst = gathered.at[s + 1 if way == 0 else n_sp - s - 1, :, part_of(h)]
        src = gathered.at[s if way == 0 else turned(s), :, part_of(h)]
        device = right if way == 0 else left
        return remote(src, dst, ring_send, ring_recv.at[way, s, h], device)

    def slots(index):
        return pl.ds(pl.multiple_of(index * cap, cap), cap)

    def row_of(kind, p, b):
        return slots((p * 2 + kind) * wide + b)

    def disp_copy(p, j, h):
        to = lax.rem(member + j, n_tp)
        return remote(
            staged.at[p, slots(to), part_of(h)],
            arrived.at[row_of(core, p, across(core)), part_of(h)],
            disp_send, disp_recv.at[p],
            device_at(core, ring, to),
        )

    def is_own(kind, b):
        return jnp.logical_and(core == kind, across(kind) == b)

    def holder(kind, b):
        return device_at(kind, z * wide + along(kind), b * 2 + kind)

    others = pl.ds(0, (n_tp - 1) * cap)
    blocks = pl.ds(0, n_sp * (n_tp - 1) // n_tp)
    peers = pl.ds(0, n_sp - 1)

    def disp_arrival(p):
        return remote(
            staged.at[p, others], arrived.at[others], disp_send, disp_recv.at[p], right
        )

    def ret_copy(kind, p, b, h):
        me = across(kind) * 2 + core
        return remote(
            results.at[row_of(kind, p, b), part_of(h)], returned.at[p, slots(me), part_of(h)],
            ret_send, ret_recv.at[p, h], holder(kind, b),
        )

    def ret_arrival(p, h):
        return remote(
            results.at[others, part_of(h)], returned.at[p, others, part_of(h)],
            ret_send, ret_recv.at[p, h], right,
        )

    def red_copy(s, way, h):
        device = left if way == 0 else right
        src = gathered.at[s if way == 0 else n_sp - s, :, part_of(h)]
        dst = (left_in if way == 0 else right_in).at[s - 1, :, part_of(h)]
        return remote(src, dst, red_send, red_recv.at[way, s - 1, h], device)

    def halo_copy(i):
        buf = (ig, cv)[i]
        device = (lax.rem(sp + 1, n_sp), tp)
        return remote(
            buf.at[pl.ds(length, HALO)], buf.at[pl.ds(0, HALO)],
            halo_send, halo_recv.at[i], device,
        )

    pieces = (pl.ds(0, HALO), pl.ds(HALO, rows - HALO))

    def conv_copy(t, i):
        return remote(
            conv_out.at[t, pieces[i]], conv_in.at[tp, pieces[i]],
            conv_send, conv_recv.at[tp], (sp, t),
        )

    def conv_arrival(t):
        return remote(conv_out.at[t], conv_in.at[t], conv_send, conv_recv.at[t], (sp, t))

    taps_count = taps.shape[0]

    def convolve(t, first, count):
        span = pl.ds(t * rows + first, count + HALO)
        mixed = ig[span].astype(jnp.float32) * cv[span].astype(jnp.float32)
        base = HALO - (taps_count - 1)
        filtered = taps[0:1, :] * mixed[base : base + count]
        for o in range(1, taps_count):
            filtered = filtered + taps[o : o + 1, :] * mixed[base + o : base + o + count]
        gate = og[pl.ds(t * rows + first, count)].astype(jnp.float32)
        conv_out[t, pl.ds(first, count)] = (gate * filtered).astype(jnp.bfloat16)

    def send_conv(t, some):
        @pl.when(tp != t)
        def _():
            for i in some:
                conv_copy(t, i).start()

    owners = [t for t in range(2, n_tp, 2)] + [t for t in range(1, n_tp, 2)]
    for copy in weights[:3] + smalls[:1]:
        copy.wait()
    for t in owners:
        convolve(t, 0, rows)
    convolve(0, HALO, rows - HALO)
    with jax.named_scope("barrier"):
        near = has_next.astype(jnp.int32) + has_last.astype(jnp.int32)
        pl.semaphore_wait(barrier, 2 + 2 * (n_tp - 1) + near)

    @pl.when(has_next)
    def _():
        halo_copy(0).start()
        halo_copy(1).start()

    for t in owners:
        send_conv(t, (1, 0))
    send_conv(0, (1,))
    for copy in weights[4:7]:
        copy.start()
    for copy in smalls[1:]:
        copy.wait()

    experts_total = n_sp * n_tp
    expert = lax.broadcasted_iota(jnp.int32, (experts_total, rows), 0)
    named = [routes[k : k + 1, :] == expert for k in range(top)]
    onehot = jnp.zeros((experts_total, rows), jnp.float32)
    for hit in named:
        onehot = jnp.where(hit, 1.0, onehot)
    earlier = lax.broadcasted_iota(jnp.int32, (rows, rows), 0) < lax.broadcasted_iota(
        jnp.int32, (rows, rows), 1
    )
    before = jnp.dot(
        onehot.astype(jnp.bfloat16),
        jnp.where(earlier, 1.0, 0.0).astype(jnp.bfloat16),
        preferred_element_type=jnp.float32,
    )

    def split(value, by):
        high = jnp.floor((value + 0.5) / by)
        return high, value - high * by

    rest, ec = split(expert.astype(jnp.float32), 2)
    rest, ey = split(rest, wide)
    ez, ex = split(rest, wide)
    turn = core.astype(jnp.float32)
    ea, eb = ex + turn * (ey - ex), ey + turn * (ex - ey)
    slot = before + ((ez * wide + ea) * n_tp + eb * 2 + ec) * cap
    metas[0] = jnp.zeros(metas.shape[1:], jnp.float32)
    for k in range(top):
        metas[0, k : k + 1, :] = jnp.sum(jnp.where(named[k], slot, 0.0), axis=0, keepdims=True)
    weight = route_weights[...]
    metas[0, top : 2 * top, :] = weight / jnp.sum(weight, axis=0, keepdims=True) * 2.5

    @pl.when(has_last)
    def _():
        with jax.named_scope("halo_wait"):
            halo_copy(0).wait_recv()
            halo_copy(1).wait_recv()

    @pl.when(jnp.logical_not(has_last))
    def _():
        for buf in (ig, cv):
            buf[pl.ds(0, HALO)] = jnp.zeros((HALO, buf.shape[1]), buf.dtype)

    convolve(0, 0, HALO)
    send_conv(0, (0,))
    weights[3].wait()
    for copy in weights[7:]:
        copy.start()

    squares = jnp.zeros((rows, 1), jnp.float32)
    product = jnp.zeros((rows, width), jnp.float32)
    part_width = conv_in.shape[2]
    gains = mix_gain[...].reshape(1, n_tp * part_width)
    sources = [tp, tp + 1 - 2 * core]
    for i in range(1, wide):
        other = lax.rem(y + i, wide) * 2
        sources += [other, other + 1]
    for i, t in enumerate(sources):
        if i == 0:
            value = conv_out[t].astype(jnp.float32)
        else:
            with jax.named_scope("conv_wait"):
                conv_arrival(t).wait_recv()
            value = conv_in[t].astype(jnp.float32)
        gain = gains[:, :part_width]
        for k in range(1, n_tp):
            gain = jnp.where(t == k, gains[:, k * part_width : (k + 1) * part_width], gain)
        squares = squares + jnp.sum(value * value, axis=1, keepdims=True)
        product = product + jnp.dot(
            (value * gain).astype(jnp.bfloat16),
            op[pl.ds(pl.multiple_of(t * part_width, part_width), part_width), :],
            preferred_element_type=jnp.float32,
        )
    inverse = lax.rsqrt(squares / (n_tp * part_width) + 1e-06)
    stream = residual[...].astype(jnp.float32) + product * inverse
    power = jnp.mean(stream * stream, axis=1, keepdims=True)
    gathered[0] = (stream * lax.rsqrt(power + 1e-06) * ffn_gain[...]).astype(jnp.bfloat16)
    total[...] = stream

    first_slot = (ring * group).astype(jnp.float32)

    def matches(meta, k):
        at = lax.broadcasted_iota(jnp.int32, (group, rows), 0).astype(jnp.float32) + first_slot
        return at == meta[k : k + 1, :]

    def dispatch(d, p, h):
        meta = metas[d]
        pick = jnp.zeros((group, rows), jnp.float32)
        for k in range(top):
            pick = jnp.where(matches(meta, k), 1.0, pick)
        staged[p, :, part_of(h)] = jnp.dot(
            pick.astype(jnp.bfloat16), gathered[d, :, part_of(h)],
            preferred_element_type=jnp.float32,
        ).astype(jnp.bfloat16)
        for j in range(1, n_tp):
            disp_copy(p, j, h).start()
        arrived[row_of(core, p, across(core)), part_of(h)] = staged[p, slots(member), part_of(h)]

    def gather_action(a):
        @pl.when(a == 0)
        def _():
            for h in range(2):
                for way in range(2):
                    if h == 0:
                        meta_copy(0, way).start()
                    ring_copy(0, way, way if h == 0 else 1 - way).start()

        @pl.when(a > 0)
        def _():
            meta_copy(a - 1, 0).wait_recv()

            @pl.when(a < half)
            def _():
                meta_copy(a, 0).start()
                meta_copy(a - 1, 1).wait_recv()

            @pl.when(a < half - 1)
            def _():
                meta_copy(a, 1).start()

            for way in range(2):
                with jax.named_scope("ring_wait"):
                    ring_copy(a - 1, way, way).wait_recv()

                @pl.when(a < half)
                def _():
                    ring_copy(a, way, way).start()

        alone = jnp.logical_or(a == 0, a == half)
        low = jnp.maximum(2 * a - 1, 0)
        ways = ((a, low), (turned(a), jnp.where(alone, low, 2 * a)))
        for way, (d, p) in enumerate(ways):
            with jax.named_scope("dispatch"):
                dispatch(d, p, way)

        @pl.when(jnp.logical_not(alone))
        def _():
            for way in range(2):
                with jax.named_scope("ring_wait"):
                    ring_copy(a - 1, way, 1 - way).wait_recv()

                @pl.when(a < half - 1)
                def _():
                    ring_copy(a, way, 1 - way).start()

            for way, (d, p) in enumerate(ways):
                with jax.named_scope("dispatch"):
                    dispatch(d, p, 1 - way)

    def run_expert(p, count):
        with jax.named_scope("disp_wait"):
            for i in range(count):
                disp_arrival(p + i).wait_recv()

        span = pl.ds(pl.multiple_of(p * 2 * batch, 2 * batch), count * 2 * batch)
        with jax.named_scope("ffn"):
            results[span] = ffn(arrived[span], eg, eu, ed).astype(jnp.bfloat16)

    def give_back(p, h):
        for kind in range(2):
            for b in range(wide):
                own = is_own(kind, b)

                @pl.when(jnp.logical_not(own))
                def _():
                    ret_copy(kind, p, b, h).start()

                @pl.when(own)
                def _():
                    returned[p, slots(member), part_of(h)] = results[
                        row_of(kind, p, b), part_of(h)
                    ]

    def combine(d, p, h):
        with jax.named_scope("ret_wait"):
            ret_arrival(p, h).wait_recv()
        meta = metas[d]
        mix = jnp.zeros((group, rows), jnp.float32)
        for k in range(top):
            mix = jnp.where(matches(meta, k), meta[top + k : top + k + 1, :], mix)
        return lax.dot_general(
            mix.astype(jnp.bfloat16), returned[p, :, part_of(h)], (((0,), (0,)), ((), ())),
            preferred_element_type=jnp.float32,
        )

    def reduce_part(s, late, first):
        for way in range(2):
            h = way if late else 1 - way
            d = s if way == 0 else n_sp - s
            parts[way] = combine(d, jnp.minimum(2 * s - 1 + way, n_sp - 1), h)

            @pl.when(first)
            def _():
                gathered[d, :, part_of(h)] = parts[way].astype(jnp.bfloat16)
                red_copy(s, way, h).start()

        @pl.when(jnp.logical_not(first))
        def _():
            for way, buf_in in enumerate((left_in, right_in)):
                h = way if late else 1 - way
                d = s if way == 0 else n_sp - s
                with jax.named_scope("red_wait"):
                    red_copy(s + 1, way, h).wait_recv()
                gathered[d, :, part_of(h)] = (
                    parts[way] + buf_in[s, :, part_of(h)].astype(jnp.float32)
                ).astype(jnp.bfloat16)
                red_copy(s, way, h).start()

    def gather_step(k, carry):
        gather_action(k)

        @pl.when(k == 0)
        def _():
            for copy in weights[4:7]:
                copy.wait()
            with jax.named_scope("shared"):
                total[...] += ffn(gathered[0], sg, su, sd)
            for copy in weights[7:]:
                copy.wait()

        @pl.when(k > 1)
        def _():
            run_expert(2 * k - 3, 2)

        @pl.when(k == half - 1)
        def _():
            give_back(n_sp - 5, 1)
            give_back(n_sp - 4, 0)

        @pl.when(k == half)
        def _():
            give_back(n_sp - 3, 1)
            give_back(n_sp - 2, 0)

        @pl.when(jnp.logical_or(k == 1, k == half))
        def _():
            run_expert(jnp.where(k == 1, 0, n_sp - 1), 1)

        return carry

    lax.fori_loop(0, half + 1, gather_step, 0)
    for h in range(2):
        give_back(n_sp - 1, h)
    remote(gathered.at[peers], gathered.at[peers], ring_send, ring_recv.at[0, 0, 0], right).wait_send()

    def reduce_step(i, carry):
        @pl.when(i < half - 1)
        def _():
            reduce_part(half - 1 - i, False, i == 0)

        s = half - 1 - i

        @pl.when(jnp.logical_and(s > 1, i > 0))
        def _():
            give_back(2 * s - 3, 1)
            give_back(2 * s - 2, 0)

        @pl.when(s > 0)
        def _():
            give_back(2 * s - 1, 0)
            give_back(2 * s, 1)

        @pl.when(s == 0)
        def _():
            give_back(0, 0)
            give_back(0, 1)

        reduce_part(half - i, True, i == 0)
        return carry

    lax.fori_loop(0, half, reduce_step, 0)
    for h in range(2):
        total[:, part_of(h)] += combine(0, 0, h)
    with jax.named_scope("drain"):
        for buf, part, sem in (
            (metas, peers, meta_send), (conv_out, pl.ds(0, n_tp - 1), conv_send),
            (staged, blocks, disp_send),
            (results, pl.ds(0, n_sp * (n_tp - 1) * cap), ret_send),
        ):
            remote(buf.at[part], buf.at[part], sem, halo_recv.at[0], right).wait_send()

        @pl.when(has_next)
        def _():
            both = conv_out.at[0, pl.ds(0, 2 * HALO)]
            remote(both, both, halo_send, halo_recv.at[0], right).wait_send()

    with jax.named_scope("red_wait_last"):
        for way in range(2):
            for h in range(2):
                red_copy(1, way, h).wait_recv()
    out[...] = (
        total[...] + left_in[0].astype(jnp.float32) + right_in[0].astype(jnp.float32)
    ).astype(out.dtype)

    with jax.named_scope("drain2"):
        remote(gathered.at[peers], gathered.at[peers], red_send, halo_recv.at[0], right).wait_send()


def body(
    out_gate,
    in_gate,
    conv_values,
    conv_taps,
    mix_gain,
    out_proj,
    residual,
    ffn_gain,
    routes,
    route_weights,
    shared_gate,
    shared_up,
    shared_down,
    expert_gate,
    expert_up,
    expert_down,
):
    n_sp, n_tp = lax.axis_size("sp"), lax.axis_size("tp")
    length, channels = in_gate.shape
    rows, width = residual.shape
    top = routes.shape[1]
    cap = max(2, 4 * rows * top // (3 * n_sp * n_tp))
    hidden, shared_hidden = expert_gate.shape[-1], shared_gate.shape[-1]
    half = n_sp // 2
    group = n_tp * cap
    wide = n_tp // 2
    bf, f32 = jnp.bfloat16, jnp.float32
    dma = pltpu.SemaphoreType.DMA
    return pl.pallas_call(
        functools.partial(experts_kernel, n_sp, n_tp, cap, top),
        out_shape=pltpu.VMEM((rows, width), bf),
        in_specs=[pl.BlockSpec(memory_space=pltpu.HBM)] * 16,
        out_specs=pl.BlockSpec(memory_space=pltpu.VMEM),
        scratch_shapes=[
            pltpu.VMEM(conv_taps.shape, f32),
            pltpu.VMEM(mix_gain.shape, f32),
            pltpu.VMEM((rows, width), bf),
            pltpu.VMEM((1, width), f32),
            pltpu.VMEM((top, rows), jnp.int32),
            pltpu.VMEM((top, rows), f32),
            pltpu.VMEM((length, channels), bf),
            pltpu.VMEM((length + HALO, channels), bf),
            pltpu.VMEM((length + HALO, channels), bf),
            pltpu.VMEM((n_tp, rows, channels), bf),
            pltpu.VMEM((n_tp, rows, channels), bf),
            pltpu.VMEM((n_sp, rows, width), bf),
            pltpu.VMEM((n_sp, META_ROWS, rows), f32),
            pltpu.VMEM((n_sp, group, width), bf),
            pltpu.VMEM((n_sp * group, width), bf),
            pltpu.VMEM((n_sp * group, width), bf),
            pltpu.VMEM((n_sp, group, width), bf),
            pltpu.VMEM((half, rows, width), bf),
            pltpu.VMEM((half, rows, width), bf),
            pltpu.VMEM((rows, width), f32),
            pltpu.VMEM((2, rows, width // 2), f32),
            pltpu.VMEM((n_tp * channels, width), bf),
            pltpu.VMEM((width, hidden), bf),
            pltpu.VMEM((width, hidden), bf),
            pltpu.VMEM((hidden, width), bf),
            pltpu.VMEM((width, shared_hidden), bf),
            pltpu.VMEM((width, shared_hidden), bf),
            pltpu.VMEM((shared_hidden, width), bf),
            dma((10,)),
            dma((6,)),
            dma(()),
            dma((2,)),
            dma(()),
            dma((n_tp,)),
            dma(()),
            dma((2, half)),
            dma(()),
            dma((2, half, 2)),
            dma(()),
            dma((n_sp,)),
            dma(()),
            dma((n_sp, 2)),
            dma(()),
            dma((2, half, 2)),
        ],
        compiler_params=pltpu.CompilerParams(
            collective_id=0, has_side_effects=True, vmem_limit_bytes=58 * 1024 * 1024
        ),
    )(
        out_gate, in_gate, conv_values, conv_taps, mix_gain,
        residual, ffn_gain.reshape(1, width), routes.T, route_weights.T,
        out_proj, expert_gate, expert_up, expert_down, shared_gate, shared_up, shared_down,
    )


def solution(mesh):
    in_specs = (
        P("sp", "tp"),
        P("sp", "tp"),
        P("sp", "tp"),
        P(None, "tp"),
        P(),
        P(),
        P(("sp", "tp"), None),
        P(),
        P(("sp", "tp"), None),
        P(("sp", "tp"), None),
        P(),
        P(),
        P(),
        P(("sp", "tp"), None, None),
        P(("sp", "tp"), None, None),
        P(("sp", "tp"), None, None),
    )
    out_specs = P(("sp", "tp"), None)
    return jax.shard_map(body, mesh=mesh, in_specs=in_specs, out_specs=out_specs, check_vma=False)
```
